512 devices in a mesh: grp: 2 (over y), fs: 32 (over z), tp: 8 (over x, core).
Axes of the slice: x: 4, y: 2, z: 32, core: 2. Of those that a mesh axis runs over, the one named last changes fastest.
The devices are a block of a 4x8x32 slice.
Arguments:
- tokens: bfloat16 [16384, 2048], P(('grp', 'fs')), parts along dimension 0, may hold values from -6 to 6
- norm_gain: float32 [2048], P('fs'), may hold values from 0.1 to 1.9
- gate_master: float32 [32, 2048, 1024], P(None, 'fs', 'tp'), may hold values from -0.125 to 0.125
- up_master: float32 [32, 2048, 1024], P(None, 'fs', 'tp'), may hold values from -0.125 to 0.125
- chosen: int32 [16384, 2], P(('grp', 'fs')), parts along dimension 0, may hold values from 0 to 31, all different within a row; in each aligned block of 256 rows (0 to 255, 256 to 511, ...) at most 32 rows name the same one
- affinity: float32 [16384, 2], P(('grp', 'fs')), parts along dimension 0, may hold values from 0.05 to 1
Outputs:
- gate_served: bfloat16 [64, 2048, 1024], P(('grp', 'fs'), None, 'tp'), parts along dimension 0
- up_served: bfloat16 [64, 2048, 1024], P(('grp', 'fs'), None, 'tp'), parts along dimension 0
- hidden: bfloat16 [16384, 2, 1024], P(('grp', 'fs'), None, 'tp'), parts along dimension 0
The draws below stay inside these ranges and needn't reach their ends.
There are 2 independent parts, one for each index of `grp`. The reference program is written for one: setup_inputs(seed, part) draws one part's arguments, and reference() takes and returns one part's arrays. A program takes and returns all parts, laid end to end along the dimension named above; an argument that names none is the same for every part. Nothing has to cross between parts.
Inputs may be any that keep to these rules, and one draw needn't show every extreme that they name: Among the rows of one index of fs (256 tokens, all their choices) no expert is chosen more than 32 times, a bound that some block reaches; the choices of one token differ.
All inputs are finite; a program needn't handle non-finite values.
Results may differ from the reference program's by a relative error of at most 0.023.
Values may be sent and summed in bfloat16 or wider, within the bound.
No kernel may reach another device: no remote copies, remote signals or barrier semaphores. Data moves between devices by JAX's collectives and lax.ppermute only.
A program may use at most 64 MiB of HBM per device.

```python
import math
import jax
import jax.numpy as jnp
import numpy as np
from jax import lax

D = 2048
F = 1024
TOP = 2
TOK_DEV = 256
EXPERTS = 32
TOKENS = 8192
CAP = 32
N_FS = 32


def levels(key, dims, shards, least, largest):
    loudness, own = 1.0, jax.random.fold_in(key, 6)
    for axis_at, blocks in shards:
        draws = jnp.exp(jax.random.uniform(jax.random.fold_in(own, axis_at), (blocks,), jnp.float32, least / len(shards), largest / len(shards)))
        loudness = loudness * jnp.repeat(draws, dims[axis_at] // blocks).reshape([-1 if axis == axis_at else 1 for axis in range(len(dims))])
    return loudness


def assign_block(rng, own, number, rows, amount, top, limit, lean):
    ranking = jax.random.permutation(rng, amount)
    crowded, ordinary = shares(amount, rows * top, limit, lean, True), shares(amount, rows * top, limit, lean, False)
    places = jnp.arange(amount)

    def named(tallies, turn):
        used = int((tallies > 0).sum())
        fixed = max(1, used // 4)
        passed = fixed + (places - fixed + turn * (used - fixed)) % max(1, amount - fixed)
        return jnp.zeros((amount,), jnp.int32).at[ranking[jnp.where(places < fixed, places, passed)]].set(jnp.asarray(tallies, jnp.int32))

    tallies = jnp.where(number % 4 == 0, named(crowded, number // 4), named(ordinary, number - number // 4 - 1))
    mixed = jax.random.permutation(jax.random.fold_in(own, 3), amount)
    giver, sink = mixed[0:amount // 2 * 2:2], mixed[1:amount // 2 * 2:2]
    slack = jnp.minimum(tallies[giver] - 1, limit - tallies[sink]) // 2
    slack = jnp.where((giver == ranking[0]) | (sink == ranking[0]) | (tallies[sink] == 0), 0, jnp.maximum(slack, 0))
    passed = jax.random.randint(jax.random.fold_in(own, 4), (amount // 2,), 0, 1 << 20) % (slack + 1)
    tallies = tallies.at[giver].add(-passed).at[sink].add(passed)
    members = jnp.searchsorted(jnp.cumsum(tallies), jnp.arange(rows * top), side="right").astype(jnp.int32)
    table = members.reshape(top, rows).T
    table = table[jax.random.permutation(jax.random.fold_in(own, 1), rows)]
    turn = jax.random.randint(jax.random.fold_in(own, 2), (rows, 1), 0, top)
    return jnp.take_along_axis(table, (jnp.arange(top)[None, :] + turn) % top, axis=1)


def shares(amount, total, most, lean, full):
    weights = [(1 << 20) // math.isqrt(grade ** lean) + 1 for grade in range(1, amount + 1)]
    largest = most if full else min(most, max(-(-total // amount), total * weights[0] // sum(weights)))
    least = 1 if total - largest >= amount - 1 else 0
    counts, rest = [largest] + [least] * (amount - 1), total - largest - least * (amount - 1)
    while rest > 0:
        candidates = [i for i in range(1, amount) if counts[i] < largest] or [i for i in range(1, amount) if counts[i] < most]
        pool, budget = sum([weights[i] for i in candidates]), rest
        for i in candidates:
            extra = min(most - counts[i], max(1, budget * weights[i] // pool), rest)
            counts[i] = counts[i] + extra
            rest = rest - extra
    return np.array(counts)


def bell_draw(own_key, shape, spread, most, split=(), kind=jnp.bfloat16):
    factor_of = levels(own_key, shape, split, -0.22, 0.18) if split else 1.0
    result = jax.random.normal(own_key, shape, jnp.float32) * spread * factor_of
    return jnp.minimum(jnp.maximum(result, -most), most).astype(kind)


def setup_inputs(seed: int = 0, part: int = 0) -> dict:
    key_of = jax.random.split(jax.random.key(seed), 7)
    part_splits = jax.random.split(jax.random.fold_in(key_of[6], part), 7)
    tokens = bell_draw(part_splits[0], (TOKENS, D), 1.0, 6.0, ((0, 32),))
    norm_gain = jnp.clip(1.0 + 0.18 * jax.random.normal(key_of[1], (D,), jnp.float32), 0.1, 1.9)
    gate_master = bell_draw(key_of[2], (EXPERTS, D, F), D ** -0.5, 0.125, ((1, 32), (2, 8)), jnp.float32)
    up_master = bell_draw(key_of[3], (EXPERTS, D, F), D ** -0.5, 0.125, ((1, 32), (2, 8)), jnp.float32)
    chosen_keys = jax.random.split(jax.random.fold_in(part_splits[4], 1), TOKENS // TOK_DEV)
    chosen_turns = jax.random.permutation(jax.random.fold_in(part_splits[4], 3), TOKENS // TOK_DEV)
    chosen = jax.vmap(lambda own, number: assign_block(jax.random.fold_in(part_splits[4], 2), own, number, TOK_DEV, EXPERTS, TOP, CAP, 2))(chosen_keys, chosen_turns).reshape((TOKENS, TOP))
    affinity = jnp.clip(jnp.exp(math.log(1.0) - 2.9957323 * jax.random.uniform(part_splits[5], (TOKENS, TOP), jnp.float32) ** levels(part_splits[5], (TOKENS, TOP), ((0, 32),), -0.2, 0.2)), 0.05, 1.0)
    return {"tokens": tokens, "norm_gain": norm_gain, "gate_master": gate_master, "up_master": up_master, "chosen": chosen, "affinity": affinity}


def reference(tokens, norm_gain, gate_master, up_master, chosen, affinity):
    gate_served = (gate_master * norm_gain[None, :, None]).astype(jnp.bfloat16)
    up_served = (up_master * norm_gain[None, :, None]).astype(jnp.bfloat16)
    xfloat = tokens.astype(jnp.float32)
    scale = lax.rsqrt(lax.optimization_barrier(jnp.mean(xfloat * xfloat, axis=-1)) + 1e-06)
    share = affinity / lax.optimization_barrier(jnp.sum(affinity, axis=-1, keepdims=True))
    blocks = chosen.reshape(N_FS, TOK_DEV * TOP)
    onehot = (blocks[:, :, None] == jnp.arange(EXPERTS, dtype=jnp.int32)[None, None, :]).astype(jnp.int32)
    slot = lax.optimization_barrier(jnp.sum((jnp.cumsum(onehot, axis=1) - onehot) * onehot, axis=2)).astype(jnp.int32)
    source = jnp.arange(N_FS, dtype=jnp.int32)[:, None]
    column = (source * CAP + slot).reshape(-1).astype(jnp.int32)
    owner = (source * TOK_DEV + jnp.repeat(jnp.arange(TOK_DEV, dtype=jnp.int32), TOP)[None, :]).reshape(-1).astype(jnp.int32)
    flat_e = blocks.reshape(-1).astype(jnp.int32)
    index_buf = jnp.zeros((EXPERTS, N_FS * CAP), jnp.int32).at[flat_e, column].set(owner)
    share_buf = jnp.zeros((EXPERTS, N_FS * CAP), jnp.float32).at[flat_e, column].set(share.reshape(-1))

    def one_expert(args):
        index, weight, w_gate, w_up = args
        rows = tokens[index]
        factor = scale[index][:, None]
        gate = jnp.dot(rows, w_gate, preferred_element_type=jnp.float32) * factor
        up = jnp.dot(rows, w_up, preferred_element_type=jnp.float32) * factor
        return (weight[:, None] * jax.nn.silu(gate) * up).astype(jnp.bfloat16)
    hidden_buf = lax.map(one_expert, (index_buf, share_buf, gate_served, up_served))
    hidden = hidden_buf[flat_e, column].reshape(TOKENS, TOP, F)
    return (gate_served, up_served, hidden)
```

```python
import functools
import jax
import jax.numpy as jnp
from jax import lax
from jax.experimental import pallas as pl
from jax.experimental.pallas import tpu as pltpu
from jax.sharding import PartitionSpec as P

F32 = jnp.float32
BF16 = jnp.bfloat16


def iota(shape, dim):
    return lax.broadcasted_iota(jnp.int32, shape, dim)


def dot(a, b, dims=(((1,), (0,)), ((), ()))):
    return lax.dot_general(a, b, dims, preferred_element_type=F32)


def pack_kernel(tokens, chosen, rows, *, experts, capacity, narrow):
    n, width = tokens.shape
    x = tokens[...].astype(F32)
    scale = lax.rsqrt(jnp.sum(x * x, axis=-1, keepdims=True) / width + 1e-06)
    at = pl.multiple_of(lax.axis_index("tp") * narrow, narrow)
    own = (tokens[:, pl.ds(at, narrow)].astype(F32) * scale).astype(BF16)
    eye = (iota((n, n), 0) == iota((n, n), 1)).astype(F32).astype(BF16)
    before = (iota((n, n), 0) < iota((n, n), 1)).astype(F32).astype(BF16)
    choice = dot(chosen[...].astype(F32).astype(BF16), eye, (((0,), (0,)), ((), ())))
    named = jnp.zeros((experts, n), F32)
    expert = iota((experts, n), 0).astype(F32)
    for k in range(chosen.shape[1]):
        named = named + (choice[k : k + 1, :] == expert).astype(F32)
    slot = dot(named.astype(BF16), before)
    slot = jnp.where(named > 0, slot, -1.0)
    pick = slot[:, None, :] == iota((experts, capacity, n), 1).astype(F32)
    pick = pick.astype(F32).reshape(experts * capacity, n).astype(BF16)
    rows[...] = dot(pick, own).astype(BF16)


def expert_kernel(parts, rows, gate, up, hidden, *, groups):
    count, sources, piece, both = parts.shape
    half = both // 2
    mine = lax.axis_index("grp")
    for q in range(count):
        at = pl.multiple_of((mine ^ q) * piece, piece)
        gate[:, pl.ds(at, piece), :] = parts[q, :, :, :half]
        up[:, pl.ds(at, piece), :] = parts[q, :, :, half:]
    slices, _, narrow = rows.shape
    block = sources * piece * count // slices
    per = gate.shape[0] // slices
    a = None
    for k in range(slices):
        w = jnp.concatenate(
            [
                gate[k * per : (k + 1) * per].reshape(block, half),
                up[k * per : (k + 1) * per].reshape(block, half),
            ],
            axis=1,
        )
        d = dot(rows[k], w)
        a = d if a is None else a + d
    g = a[:, :half]
    hidden[...] = (g / (1.0 + jnp.exp(-g)) * a[:, half:]).astype(BF16)


def pick_kernel(back, chosen, affinity, out, *, experts, capacity):
    n, top = chosen.shape
    total = back.shape[0]
    c = chosen[...]
    lane = iota((n, experts), 1)
    hot = [(c[:, k : k + 1] == lane).astype(F32) for k in range(top)]
    named = functools.reduce(jnp.add, hot)
    before = (iota((n, n), 1) < iota((n, n), 0)).astype(F32).astype(BF16)
    slot = dot(before, named.astype(BF16))
    a = affinity[...]
    share = a / jnp.sum(a, axis=-1, keepdims=True)
    slots = iota((n, total), 1)
    for k in range(top):
        at = jnp.sum(hot[k] * slot, axis=1, keepdims=True).astype(jnp.int32)
        at = at + c[:, k : k + 1] * capacity
        take = (slots == at).astype(F32).astype(BF16)
        out[:, k, :] = (dot(take, back[...]) * share[:, k : k + 1]).astype(BF16)


def on_device(tokens, norm_gain, gate_master, up_master, chosen, affinity):
    groups, sources, slices = (lax.axis_size(a) for a in ("grp", "fs", "tp"))
    experts, block, half = gate_master.shape
    n, width = tokens.shape
    top = chosen.shape[1]
    capacity = n * top * 2 // experts
    narrow = width // slices
    piece = block // groups
    vmem = pl.BlockSpec(memory_space=pltpu.VMEM)

    rows = pl.pallas_call(
        functools.partial(pack_kernel, experts=experts, capacity=capacity, narrow=narrow),
        out_shape=jax.ShapeDtypeStruct((experts * capacity, narrow), BF16),
        in_specs=[vmem, vmem],
        out_specs=vmem,
        name="pack",
    )(tokens, chosen)
    rows = lax.all_to_all(
        rows.reshape(experts, capacity, narrow), "fs", split_axis=0, concat_axis=0, tiled=True
    )
    rows = rows.reshape(experts * capacity, narrow)

    at = lax.axis_index("grp") * piece
    gain = lax.dynamic_slice_in_dim(norm_gain, at, piece, 0)[None, :, None]
    folded = jnp.concatenate(
        [
            (lax.dynamic_slice_in_dim(m, at, piece, 1) * gain).astype(BF16)
            for m in (gate_master, up_master)
        ],
        axis=2,
    )
    folded, rows = lax.optimization_barrier((folded, rows))
    every = lax.all_gather(rows, "tp", axis=0, tiled=False)
    got = lax.all_to_all(folded, "fs", split_axis=0, concat_axis=0, tiled=True)[None]
    step = 1
    while step < groups:
        swap = [(i, i ^ step) for i in range(groups)]
        got = jnp.concatenate([got, lax.ppermute(got, "grp", swap)], axis=0)
        step *= 2

    gate, up, hidden = pl.pallas_call(
        functools.partial(expert_kernel, groups=groups),
        out_shape=(
            jax.ShapeDtypeStruct((sources, block, half), BF16),
            jax.ShapeDtypeStruct((sources, block, half), BF16),
            jax.ShapeDtypeStruct((experts * capacity, half), BF16),
        ),
        in_specs=[vmem, vmem],
        out_specs=(vmem, vmem, vmem),
        name="experts",
    )(got, every)
    back = lax.all_to_all(
        hidden.reshape(experts, capacity, half), "fs", split_axis=0, concat_axis=0, tiled=True
    )
    out = pl.pallas_call(
        functools.partial(pick_kernel, experts=experts, capacity=capacity),
        out_shape=jax.ShapeDtypeStruct((n, top, half), BF16),
        in_specs=[vmem, vmem, vmem],
        out_specs=vmem,
        name="pick",
    )(back.reshape(experts * capacity, half), chosen, affinity)
    return (
        gate.reshape(1, sources * block, half),
        up.reshape(1, sources * block, half),
        out,
    )


def solution(mesh):
    return jax.shard_map(
        on_device,
        mesh=mesh,
        in_specs=(
            P(("grp", "fs"), None),
            P("fs"),
            P(None, "fs", "tp"),
            P(None, "fs", "tp"),
            P(("grp", "fs"), None),
            P(("grp", "fs"), None),
        ),
        out_specs=(
            P(("grp", "fs"), None, "tp"),
            P(("grp", "fs"), None, "tp"),
            P(("grp", "fs"), None, "tp"),
        ),
        check_vma=False,
    )
```

```python
import functools
import jax
import jax.numpy as jnp
from jax import lax
from jax.experimental import pallas as pl
from jax.experimental.pallas import tpu as pltpu
from jax.sharding import PartitionSpec as P

F32 = jnp.float32
BF16 = jnp.bfloat16
CORES = 2
TILE = 8


def iota(shape, dim):
    return lax.broadcasted_iota(jnp.int32, shape, dim)


def dot(a, b, dims=(((1,), (0,)), ((), ()))):
    return lax.dot_general(a, b, dims, preferred_element_type=F32)


def column(row):
    n = row.shape[1]
    return jnp.sum(jnp.where(iota((n, n), 0) == iota((n, n), 1), row, 0.0), axis=1, keepdims=True)


def slots_of(choice, experts):
    top, n = choice.shape
    expert = iota((experts, n), 0).astype(F32)
    named = jnp.zeros((experts, n), F32)
    for k in range(top):
        named = named + (choice[k : k + 1, :] == expert).astype(F32)
    before = (iota((n, n), 0) < iota((n, n), 1)).astype(F32).astype(BF16)
    return named, dot(named.astype(BF16), before)


def pack_kernel(tokens, chosen, gain, gate, up, out, gains, *, experts, capacity, narrow, piece):
    n, width = tokens.shape
    x = tokens[...].astype(F32)
    scale = lax.rsqrt(jnp.sum(x * x, axis=-1, keepdims=True) / width + 1e-06)
    at = pl.multiple_of(lax.axis_index("tp") * narrow, narrow)
    own = (tokens[:, pl.ds(at, narrow)].astype(F32) * scale).astype(BF16)
    named, slot = slots_of(chosen[...].astype(F32), experts)
    slot = jnp.where(named > 0, slot, -1.0)
    pick = slot[:, None, :] == iota((experts, capacity, n), 1).astype(F32)
    pick = pick.astype(F32).reshape(experts * capacity, n).astype(BF16)
    out[:, :capacity, :] = dot(pick, own).astype(BF16).reshape(experts, capacity, narrow)
    rows = out.shape[1] - capacity
    if rows:
        half = gate.shape[2]
        gains[...] = jnp.broadcast_to(column(gain[...]), gains.shape)
        at = pl.multiple_of(lax.axis_index("grp") * piece, TILE)
        g = gains[pl.ds(at, rows), :][None]
        out[:, capacity:, :half] = (gate[:, pl.ds(at, rows), :] * g).astype(BF16)
        out[:, capacity:, half:] = (up[:, pl.ds(at, rows), :] * g).astype(BF16)


def expert_kernel(*refs, shares, cores):
    gate, up, hidden = refs[-3:]
    weights = refs[: sum(count for count, _ in shares)]
    slices = refs[len(weights) : -3]
    half = gate.shape[2]
    mine = lax.axis_index("grp")
    piece = sum(rows for _, rows in shares_rows(shares, weights))
    first = 0
    start = 0
    for count, _ in shares:
        group = weights[start : start + count]
        rows = group[0].shape[2]
        q = 0
        for ref in group:
            for j in range(ref.shape[0]):
                at = pl.multiple_of((mine ^ q) * piece + first, TILE)
                gate[:, pl.ds(at, rows), :] = ref[j, :, :, :half]
                up[:, pl.ds(at, rows), :] = ref[j, :, :, half:]
                q += 1
        first += rows
        start += count
    total = len(slices)
    per = gate.shape[0] // total
    block = per * gate.shape[1]
    tp = lax.axis_index("tp")
    a = None
    for ref, where in zip(slices, slice_places(total, cores)):
        at = where(tp) * per
        w = jnp.concatenate(
            [
                gate[pl.ds(at, per)].reshape(block, half),
                up[pl.ds(at, per)].reshape(block, half),
            ],
            axis=1,
        )
        d = dot(ref[...], w)
        a = d if a is None else a + d
    g = a[:, :half]
    hidden[...] = (g / (1.0 + jnp.exp(-g)) * a[:, half:]).astype(BF16)


def shares_rows(shares, weights):
    start = 0
    for count, _ in shares:
        yield count, weights[start].shape[2]
        start += count


def pick_kernel(back, chosen, affinity, out, *, experts, capacity):
    top, n = chosen.shape
    total = back.shape[0]
    choice = chosen[...].astype(F32)
    named, slot = slots_of(choice, experts)
    expert = iota((experts, n), 0).astype(F32)
    a = affinity[...]
    share = a / jnp.sum(a, axis=0, keepdims=True)
    slots = iota((total, n), 0).astype(F32)
    for k in range(top):
        c = choice[k : k + 1, :]
        at = jnp.sum(jnp.where(c == expert, slot, 0.0), axis=0, keepdims=True) + c * capacity
        take = (slots == at).astype(F32).astype(BF16)
        got = dot(take, back[...], (((0,), (0,)), ((), ())))
        out[:, k, :] = (got * column(share[k : k + 1, :])).astype(BF16)


def ring_tables(total, cores):
    def hop(sign):
        def to(i):
            turn = sign if i % cores == 0 else -sign
            return (i + turn * cores) % total

        return [(i, to(i)) for i in range(total)]

    return hop(1), hop(-1), [(i, i ^ 1) for i in range(total)]


def slice_places(total, cores):
    chips = total // cores

    def away(steps):
        def place(i):
            turn = jnp.where(i % cores == 0, -steps, steps)
            return (i + turn * cores + total) % total

        return place

    places = [away(0)]
    for s in range(1, chips // 2 + 1):
        places.append(away(s))
        if s <= (chips - 1) // 2:
            places.append(away(-s))
    return places + [lambda i, p=p: p(i ^ 1) for p in places]


def gather_slices(own, total, cores):
    ahead, behind, swap = ring_tables(total, cores)
    chips = total // cores
    got = [own]
    one = two = own
    for s in range(1, chips // 2 + 1):
        one = lax.ppermute(one, "tp", ahead)
        got.append(one)
        if s <= (chips - 1) // 2:
            two = lax.ppermute(two, "tp", behind)
            got.append(two)
    return got + [lax.ppermute(g, "tp", swap) for g in got]


def gather_groups(own, groups):
    got = [own]
    step = 1
    while step < groups:
        send = got[0] if len(got) == 1 else jnp.concatenate(got, axis=0)
        got.append(lax.ppermute(send, "grp", [(i, i ^ step) for i in range(groups)]))
        step *= 2
    return got


def on_device(tokens, norm_gain, gate_master, up_master, chosen, affinity):
    groups, sources, total = (lax.axis_size(a) for a in ("grp", "fs", "tp"))
    experts, block, half = gate_master.shape
    n, width = tokens.shape
    top = chosen.shape[1]
    capacity = n * top * 2 // experts
    narrow = width // total
    piece = block // groups
    late = piece // 2 // TILE * TILE
    early = piece - late
    vmem = pl.BlockSpec(memory_space=pltpu.VMEM)

    sent = pl.pallas_call(
        functools.partial(
            pack_kernel, experts=experts, capacity=capacity, narrow=narrow, piece=piece
        ),
        out_shape=jax.ShapeDtypeStruct((experts, capacity + early, narrow), BF16),
        in_specs=[vmem] * 5,
        out_specs=vmem,
        scratch_shapes=[pltpu.VMEM((block, half), F32)],
        name="pack",
    )(tokens, chosen.T, norm_gain[None, :], gate_master, up_master)
    got = lax.all_to_all(sent, "fs", split_axis=0, concat_axis=0, tiled=True)
    rows = got[:, :capacity, :].reshape(sources * capacity, narrow)
    weights = [gather_groups(got[None, :, capacity:, :], groups)]
    if late:
        at = lax.axis_index("grp") * piece + early
        gain = lax.dynamic_slice_in_dim(norm_gain, at, late, 0)[None, :, None]
        folded = jnp.concatenate(
            [
                (lax.dynamic_slice_in_dim(m, at, late, 1) * gain).astype(BF16)
                for m in (gate_master, up_master)
            ],
            axis=2,
        )
        folded, rows = lax.optimization_barrier((folded, rows))
        more = lax.all_to_all(folded, "fs", split_axis=0, concat_axis=0, tiled=True)
        weights.append(gather_groups(more[None], groups))
    slices = gather_slices(rows, total, CORES)
    shares = tuple((len(w), 0) for w in weights)
    flat = [w for part in weights for w in part]

    gate, up, hidden = pl.pallas_call(
        functools.partial(expert_kernel, shares=shares, cores=CORES),
        out_shape=(
            jax.ShapeDtypeStruct((sources, block, half), BF16),
            jax.ShapeDtypeStruct((sources, block, half), BF16),
            jax.ShapeDtypeStruct((sources * capacity, half), BF16),
        ),
        in_specs=[vmem] * (len(flat) + len(slices)),
        out_specs=(vmem, vmem, vmem),
        name="experts",
    )(*flat, *slices)
    back = lax.all_to_all(
        hidden.reshape(sources, capacity, half), "fs", split_axis=0, concat_axis=0, tiled=True
    )
    out = pl.pallas_call(
        functools.partial(pick_kernel, experts=experts, capacity=capacity),
        out_shape=jax.ShapeDtypeStruct((n, top, half), BF16),
        in_specs=[vmem, vmem, vmem],
        out_specs=vmem,
        name="pick",
    )(back.reshape(experts * capacity, half), chosen.T, affinity.T)
    return (
        gate.reshape(1, sources * block, half),
        up.reshape(1, sources * block, half),
        out,
    )


def solution(mesh):
    return jax.shard_map(
        on_device,
        mesh=mesh,
        in_specs=(
            P(("grp", "fs"), None),
            P("fs"),
            P(None, "fs", "tp"),
            P(None, "fs", "tp"),
            P(("grp", "fs"), None),
            P(("grp", "fs"), None),
        ),
        out_specs=(
            P(("grp", "fs"), None, "tp"),
            P(("grp", "fs"), None, "tp"),
            P(("grp", "fs"), None, "tp"),
        ),
        check_vma=False,
    )
```

```python
import functools
import jax
import jax.numpy as jnp
from jax import lax
from jax.experimental import pallas as pl
from jax.experimental.pallas import tpu as pltpu
from jax.sharding import PartitionSpec as P

F32 = jnp.float32
BF16 = jnp.bfloat16
CORES = 2
TILE = 8


def iota(shape, dim):
    return lax.broadcasted_iota(jnp.int32, shape, dim)


def dot(a, b, dims=(((1,), (0,)), ((), ()))):
    return lax.dot_general(a, b, dims, preferred_element_type=F32)


def column(row):
    n = row.shape[1]
    return jnp.sum(jnp.where(iota((n, n), 0) == iota((n, n), 1), row, 0.0), axis=1, keepdims=True)


def slots_of(choice, experts):
    top, n = choice.shape
    expert = iota((experts, n), 0).astype(F32)
    named = jnp.zeros((experts, n), F32)
    for k in range(top):
        named = named + (choice[k : k + 1, :] == expert).astype(F32)
    before = (iota((n, n), 0) < iota((n, n), 1)).astype(F32).astype(BF16)
    return named, dot(named.astype(BF16), before)


def pack_kernel(tokens, chosen, gain, gate, up, out, gains, *, experts, capacity, narrow, piece):
    n, width = tokens.shape
    x = tokens[...].astype(F32)
    scale = lax.rsqrt(jnp.sum(x * x, axis=-1, keepdims=True) / width + 1e-06)
    at = pl.multiple_of(lax.axis_index("tp") * narrow, narrow)
    own = (tokens[:, pl.ds(at, narrow)].astype(F32) * scale).astype(BF16)
    named, slot = slots_of(chosen[...].astype(F32), experts)
    slot = jnp.where(named > 0, slot, -1.0)
    pick = slot[:, None, :] == iota((experts, capacity, n), 1).astype(F32)
    pick = pick.astype(F32).reshape(experts * capacity, n).astype(BF16)
    out[:, :capacity, :] = dot(pick, own).astype(BF16).reshape(experts, capacity, narrow)
    rows = out.shape[1] - capacity
    if rows:
        half = gate.shape[2]
        gains[...] = jnp.broadcast_to(column(gain[...]), gains.shape)
        at = pl.multiple_of(lax.axis_index("grp") * piece, TILE)
        g = gains[pl.ds(at, rows), :][None]
        out[:, capacity:, :half] = (gate[:, pl.ds(at, rows), :] * g).astype(BF16)
        out[:, capacity:, half:] = (up[:, pl.ds(at, rows), :] * g).astype(BF16)


def expert_kernel(*refs, shares, cores):
    gate, up, hidden = refs[-3:]
    weights = refs[: sum(count for count, _ in shares)]
    slices = refs[len(weights) : -3]
    half = gate.shape[2]
    mine = lax.axis_index("grp")
    piece = sum(rows for _, rows in shares_rows(shares, weights))
    first = 0
    start = 0
    for count, _ in shares:
        group = weights[start : start + count]
        rows = group[0].shape[2]
        q = 0
        for ref in group:
            for j in range(ref.shape[0]):
                at = pl.multiple_of((mine ^ q) * piece + first, TILE)
                gate[:, pl.ds(at, rows), :] = ref[j, :, :, :half]
                up[:, pl.ds(at, rows), :] = ref[j, :, :, half:]
                q += 1
        first += rows
        start += count
    total = len(slices)
    per = gate.shape[0] // total
    block = per * gate.shape[1]
    tp = lax.axis_index("tp")
    a = None
    for ref, where in zip(slices, slice_places(total, cores)):
        at = where(tp) * per
        w = jnp.concatenate(
            [
                gate[pl.ds(at, per)].reshape(block, half),
                up[pl.ds(at, per)].reshape(block, half),
            ],
            axis=1,
        )
        d = dot(ref[...], w)
        a = d if a is None else a + d
    g = a[:, :half]
    hidden[...] = (g / (1.0 + jnp.exp(-g)) * a[:, half:]).astype(BF16)


def shares_rows(shares, weights):
    start = 0
    for count, _ in shares:
        yield count, weights[start].shape[2]
        start += count


def place_kernel(chosen, affinity, take, share, *, experts, capacity):
    top, n = chosen.shape
    total = take.shape[1]
    choice = chosen[...].astype(F32)
    named, slot = slots_of(choice, experts)
    expert = iota((experts, n), 0).astype(F32)
    a = affinity[...]
    part = a / jnp.sum(a, axis=0, keepdims=True)
    slots = iota((total, n), 0).astype(F32)
    for k in range(top):
        c = choice[k : k + 1, :]
        at = jnp.sum(jnp.where(c == expert, slot, 0.0), axis=0, keepdims=True) + c * capacity
        take[k] = (slots == at).astype(F32).astype(BF16)
        share[k] = jnp.broadcast_to(column(part[k : k + 1, :]), share.shape[1:])


def pick_kernel(back, take, share, out):
    for k in range(take.shape[0]):
        got = dot(take[k], back[...], (((0,), (0,)), ((), ())))
        out[:, k, :] = (got * share[k]).astype(BF16)


def ring_tables(total, cores):
    def hop(sign):
        def to(i):
            turn = sign if i % cores == 0 else -sign
            return (i + turn * cores) % total

        return [(i, to(i)) for i in range(total)]

    return hop(1), hop(-1), [(i, i ^ 1) for i in range(total)]


def slice_places(total, cores):
    chips = total // cores

    def away(steps):
        def place(i):
            turn = jnp.where(i % cores == 0, -steps, steps)
            return (i + turn * cores + total) % total

        return place

    places = [away(0)]
    for s in range(1, chips // 2 + 1):
        places.append(away(s))
        if s <= (chips - 1) // 2:
            places.append(away(-s))
    return places + [lambda i, p=p: p(i ^ 1) for p in places]


def gather_slices(own, total, cores):
    ahead, behind, swap = ring_tables(total, cores)
    chips = total // cores
    got = [own]
    one = two = own
    for s in range(1, chips // 2 + 1):
        one = lax.ppermute(one, "tp", ahead)
        got.append(one)
        if s <= (chips - 1) // 2:
            two = lax.ppermute(two, "tp", behind)
            got.append(two)
    return got + [lax.ppermute(g, "tp", swap) for g in got]


def gather_groups(own, groups):
    got = [own]
    step = 1
    while step < groups:
        send = got[0] if len(got) == 1 else jnp.concatenate(got, axis=0)
        got.append(lax.ppermute(send, "grp", [(i, i ^ step) for i in range(groups)]))
        step *= 2
    return got


def on_device(tokens, norm_gain, gate_master, up_master, chosen, affinity):
    groups, sources, total = (lax.axis_size(a) for a in ("grp", "fs", "tp"))
    experts, block, half = gate_master.shape
    n, width = tokens.shape
    top = chosen.shape[1]
    capacity = n * top * 2 // experts
    narrow = width // total
    piece = block // groups
    late = piece // 2 // TILE * TILE
    early = piece - late
    vmem = pl.BlockSpec(memory_space=pltpu.VMEM)

    sent = pl.pallas_call(
        functools.partial(
            pack_kernel, experts=experts, capacity=capacity, narrow=narrow, piece=piece
        ),
        out_shape=jax.ShapeDtypeStruct((experts, capacity + early, narrow), BF16),
        in_specs=[vmem] * 5,
        out_specs=vmem,
        scratch_shapes=[pltpu.VMEM((block, half), F32)],
        name="pack",
    )(tokens, chosen.T, norm_gain[None, :], gate_master, up_master)
    got = lax.all_to_all(sent, "fs", split_axis=0, concat_axis=0, tiled=True)
    rows = got[:, :capacity, :].reshape(sources * capacity, narrow)
    weights = [gather_groups(got[None, :, capacity:, :], groups)]
    if late:
        at = lax.axis_index("grp") * piece + early
        gain = lax.dynamic_slice_in_dim(norm_gain, at, late, 0)[None, :, None]
        folded = jnp.concatenate(
            [
                (lax.dynamic_slice_in_dim(m, at, late, 1) * gain).astype(BF16)
                for m in (gate_master, up_master)
            ],
            axis=2,
        )
        folded, rows = lax.optimization_barrier((folded, rows))
        more = lax.all_to_all(folded, "fs", split_axis=0, concat_axis=0, tiled=True)
        weights.append(gather_groups(more[None], groups))
    slices = gather_slices(rows, total, CORES)
    shares = tuple((len(w), 0) for w in weights)
    flat = [w for part in weights for w in part]

    gate, up, hidden = pl.pallas_call(
        functools.partial(expert_kernel, shares=shares, cores=CORES),
        out_shape=(
            jax.ShapeDtypeStruct((sources, block, half), BF16),
            jax.ShapeDtypeStruct((sources, block, half), BF16),
            jax.ShapeDtypeStruct((sources * capacity, half), BF16),
        ),
        in_specs=[vmem] * (len(flat) + len(slices)),
        out_specs=(vmem, vmem, vmem),
        name="experts",
    )(*flat, *slices)
    hidden, choice, ratio = lax.optimization_barrier((hidden, chosen.T, affinity.T))
    back = lax.all_to_all(
        hidden.reshape(sources, capacity, half), "fs", split_axis=0, concat_axis=0, tiled=True
    )
    take, share = pl.pallas_call(
        functools.partial(place_kernel, experts=experts, capacity=capacity),
        out_shape=(
            jax.ShapeDtypeStruct((top, experts * capacity, n), BF16),
            jax.ShapeDtypeStruct((top, n, half), F32),
        ),
        in_specs=[vmem] * 2,
        out_specs=(vmem, vmem),
        name="place",
    )(choice, ratio)
    out = pl.pallas_call(
        pick_kernel,
        out_shape=jax.ShapeDtypeStruct((n, top, half), BF16),
        in_specs=[vmem] * 3,
        out_specs=vmem,
        name="pick",
    )(back.reshape(experts * capacity, half), take, share)
    return (
        gate.reshape(1, sources * block, half),
        up.reshape(1, sources * block, half),
        out,
    )


def solution(mesh):
    return jax.shard_map(
        on_device,
        mesh=mesh,
        in_specs=(
            P(("grp", "fs"), None),
            P("fs"),
            P(None, "fs", "tp"),
            P(None, "fs", "tp"),
            P(("grp", "fs"), None),
            P(("grp", "fs"), None),
        ),
        out_specs=(
            P(("grp", "fs"), None, "tp"),
            P(("grp", "fs"), None, "tp"),
            P(("grp", "fs"), None, "tp"),
        ),
        check_vma=False,
    )
```

```python
import functools
import jax
import jax.numpy as jnp
from jax import lax
from jax.experimental import pallas as pl
from jax.experimental.pallas import tpu as pltpu
from jax.sharding import PartitionSpec as P

F32 = jnp.float32
BF16 = jnp.bfloat16
CORES = 2
TILE = 8


def iota(shape, dim):
    return lax.broadcasted_iota(jnp.int32, shape, dim)


def dot(a, b, dims=(((1,), (0,)), ((), ()))):
    return lax.dot_general(a, b, dims, preferred_element_type=F32)


def column(row):
    n = row.shape[1]
    return jnp.sum(jnp.where(iota((n, n), 0) == iota((n, n), 1), row, 0.0), axis=1, keepdims=True)


def slots_of(choice, experts):
    top, n = choice.shape
    expert = iota((experts, n), 0).astype(F32)
    named = jnp.zeros((experts, n), F32)
    for k in range(top):
        named = named + (choice[k : k + 1, :] == expert).astype(F32)
    before = (iota((n, n), 0) < iota((n, n), 1)).astype(F32).astype(BF16)
    return named, dot(named.astype(BF16), before)


def pack_kernel(tokens, chosen, gain, gate, up, out, gains, *, experts, capacity, narrow, piece):
    n, width = tokens.shape
    x = tokens[...].astype(F32)
    scale = lax.rsqrt(jnp.sum(x * x, axis=-1, keepdims=True) / width + 1e-06)
    at = pl.multiple_of(lax.axis_index("tp") * narrow, narrow)
    own = (tokens[:, pl.ds(at, narrow)].astype(F32) * scale).astype(BF16)
    named, slot = slots_of(chosen[...].astype(F32), experts)
    slot = jnp.where(named > 0, slot, -1.0)
    pick = slot[:, None, :] == iota((experts, capacity, n), 1).astype(F32)
    pick = pick.astype(F32).reshape(experts * capacity, n).astype(BF16)
    out[:, :capacity, :] = dot(pick, own).astype(BF16).reshape(experts, capacity, narrow)
    half = gate.shape[2]
    gains[...] = jnp.broadcast_to(column(gain[...]), gains.shape)
    at = pl.multiple_of(lax.axis_index("grp") * piece, TILE)
    g = gains[pl.ds(at, piece), :][None]
    out[:, capacity:, :half] = (gate[:, pl.ds(at, piece), :] * g).astype(BF16)
    out[:, capacity:, half:] = (up[:, pl.ds(at, piece), :] * g).astype(BF16)


def expert_kernel(*refs, parts, cores):
    gate, up, hidden = refs[-3:]
    weights, slices = refs[:parts], refs[parts:-3]
    half = gate.shape[2]
    piece = weights[0].shape[2]
    mine = lax.axis_index("grp")
    q = 0
    for ref in weights:
        for j in range(ref.shape[0]):
            at = pl.multiple_of((mine ^ q) * piece, TILE)
            gate[:, pl.ds(at, piece), :] = ref[j, :, :, :half]
            up[:, pl.ds(at, piece), :] = ref[j, :, :, half:]
            q += 1
    total = len(slices)
    per = gate.shape[0] // total
    block = per * gate.shape[1]
    tp = lax.axis_index("tp")
    a = None
    for ref, where in zip(slices, slice_places(total, cores)):
        at = where(tp) * per
        w = jnp.concatenate(
            [
                gate[pl.ds(at, per)].reshape(block, half),
                up[pl.ds(at, per)].reshape(block, half),
            ],
            axis=1,
        )
        d = dot(ref[...], w)
        a = d if a is None else a + d
    g = a[:, :half]
    hidden[...] = (g / (1.0 + jnp.exp(-g)) * a[:, half:]).astype(BF16)


def place_kernel(chosen, affinity, take, share, *, experts, capacity):
    top, n = chosen.shape
    total = take.shape[2]
    choice = chosen[...].astype(F32)
    named, slot = slots_of(choice, experts)
    expert = iota((experts, n), 0).astype(F32)
    a = affinity[...]
    part = a / jnp.sum(a, axis=0, keepdims=True)
    slots = iota((n, total), 1).astype(F32)
    for k in range(top):
        c = choice[k : k + 1, :]
        at = jnp.sum(jnp.where(c == expert, slot, 0.0), axis=0, keepdims=True) + c * capacity
        take[k] = (slots == column(at)).astype(F32).astype(BF16)
        share[k] = jnp.broadcast_to(column(part[k : k + 1, :]), share.shape[1:])


def pick_kernel(back, take, share, out):
    for k in range(take.shape[0]):
        out[:, k, :] = (dot(take[k], back[...]) * share[k]).astype(BF16)


def ring_tables(total, cores):
    def hop(sign):
        def to(i):
            turn = sign if i % cores == 0 else -sign
            return (i + turn * cores) % total

        return [(i, to(i)) for i in range(total)]

    return hop(1), hop(-1), [(i, i ^ 1) for i in range(total)]


def slice_places(total, cores):
    chips = total // cores

    def away(steps):
        def place(i):
            turn = jnp.where(i % cores == 0, -steps, steps)
            return (i + turn * cores + total) % total

        return place

    places = [away(0)]
    for s in range(1, chips // 2 + 1):
        places.append(away(s))
        if s <= (chips - 1) // 2:
            places.append(away(-s))
    return places + [lambda i, p=p: p(i ^ 1) for p in places]


def gather_slices(own, total, cores):
    ahead, behind, swap = ring_tables(total, cores)
    chips = total // cores
    got = [own]
    one = two = own
    for s in range(1, chips // 2 + 1):
        one = lax.ppermute(one, "tp", ahead)
        got.append(one)
        if s <= (chips - 1) // 2:
            two = lax.ppermute(two, "tp", behind)
            got.append(two)
    return got + [lax.ppermute(g, "tp", swap) for g in got]


def gather_groups(own, groups):
    got = [own]
    step = 1
    while step < groups:
        send = got[0] if len(got) == 1 else jnp.concatenate(got, axis=0)
        got.append(lax.ppermute(send, "grp", [(i, i ^ step) for i in range(groups)]))
        step *= 2
    return got


def on_device(tokens, norm_gain, gate_master, up_master, chosen, affinity):
    groups, sources, total = (lax.axis_size(a) for a in ("grp", "fs", "tp"))
    experts, block, half = gate_master.shape
    n, width = tokens.shape
    top = chosen.shape[1]
    capacity = n * top * 2 // experts
    narrow = width // total
    piece = block // groups
    vmem = pl.BlockSpec(memory_space=pltpu.VMEM)

    sent = pl.pallas_call(
        functools.partial(
            pack_kernel, experts=experts, capacity=capacity, narrow=narrow, piece=piece
        ),
        out_shape=jax.ShapeDtypeStruct((experts, capacity + piece, narrow), BF16),
        in_specs=[vmem] * 5,
        out_specs=vmem,
        scratch_shapes=[pltpu.VMEM((block, half), F32)],
        name="pack",
    )(tokens, chosen.T, norm_gain[None, :], gate_master, up_master)
    got = lax.all_to_all(sent, "fs", split_axis=0, concat_axis=0, tiled=True)
    rows = got[:, :capacity, :].reshape(sources * capacity, narrow)
    weights = gather_groups(got[None, :, capacity:, :], groups)
    slices = gather_slices(rows, total, CORES)

    gate, up, hidden = pl.pallas_call(
        functools.partial(expert_kernel, parts=len(weights), cores=CORES),
        out_shape=(
            jax.ShapeDtypeStruct((sources, block, half), BF16),
            jax.ShapeDtypeStruct((sources, block, half), BF16),
            jax.ShapeDtypeStruct((sources * capacity, half), BF16),
        ),
        in_specs=[vmem] * (len(weights) + len(slices)),
        out_specs=(vmem, vmem, vmem),
        name="experts",
    )(*weights, *slices)
    hidden, choice, ratio = lax.optimization_barrier((hidden, chosen.T, affinity.T))
    back = lax.all_to_all(
        hidden.reshape(sources, capacity, half), "fs", split_axis=0, concat_axis=0, tiled=True
    )
    take, share = pl.pallas_call(
        functools.partial(place_kernel, experts=experts, capacity=capacity),
        out_shape=(
            jax.ShapeDtypeStruct((top, n, experts * capacity), BF16),
            jax.ShapeDtypeStruct((top, n, half), F32),
        ),
        in_specs=[vmem] * 2,
        out_specs=(vmem, vmem),
        name="place",
    )(choice, ratio)
    out = pl.pallas_call(
        pick_kernel,
        out_shape=jax.ShapeDtypeStruct((n, top, half), BF16),
        in_specs=[vmem] * 3,
        out_specs=vmem,
        name="pick",
    )(back.reshape(experts * capacity, half), take, share)
    return (
        gate.reshape(1, sources * block, half),
        up.reshape(1, sources * block, half),
        out,
    )


def solution(mesh):
    return jax.shard_map(
        on_device,
        mesh=mesh,
        in_specs=(
            P(("grp", "fs"), None),
            P("fs"),
            P(None, "fs", "tp"),
            P(None, "fs", "tp"),
            P(("grp", "fs"), None),
            P(("grp", "fs"), None),
        ),
        out_specs=(
            P(("grp", "fs"), None, "tp"),
            P(("grp", "fs"), None, "tp"),
            P(("grp", "fs"), None, "tp"),
        ),
        check_vma=False,
    )
```

```python
import functools
import jax
import jax.numpy as jnp
from jax import lax
from jax.experimental import pallas as pl
from jax.experimental.pallas import tpu as pltpu
from jax.sharding import PartitionSpec as P

F32 = jnp.float32
BF16 = jnp.bfloat16
CORES = 2
TILE = 8
STEPS = 4


def iota(shape, dim):
    return lax.broadcasted_iota(jnp.int32, shape, dim)


def dot(a, b, dims=(((1,), (0,)), ((), ()))):
    return lax.dot_general(a, b, dims, preferred_element_type=F32)


def column(row):
    n = row.shape[1]
    return jnp.sum(jnp.where(iota((n, n), 0) == iota((n, n), 1), row, 0.0), axis=1, keepdims=True)


def slots_of(choice, experts):
    top, n = choice.shape
    expert = iota((experts, n), 0).astype(F32)
    named = jnp.zeros((experts, n), F32)
    for k in range(top):
        named = named + (choice[k : k + 1, :] == expert).astype(F32)
    before = (iota((n, n), 0) < iota((n, n), 1)).astype(F32).astype(BF16)
    return named, dot(named.astype(BF16), before)


def pack_kernel(tokens, chosen, gain, gate, up, out, gains, *, experts, capacity, narrow, piece):
    n, width = tokens.shape
    x = tokens[...].astype(F32)
    scale = lax.rsqrt(jnp.sum(x * x, axis=-1, keepdims=True) / width + 1e-06)
    at = pl.multiple_of(lax.axis_index("tp") * narrow, narrow)
    own = (tokens[:, pl.ds(at, narrow)].astype(F32) * scale).astype(BF16)
    named, slot = slots_of(chosen[...].astype(F32), experts)
    slot = jnp.where(named > 0, slot, -1.0)
    pick = slot[:, None, :] == iota((experts, capacity, n), 1).astype(F32)
    pick = pick.astype(F32).reshape(experts * capacity, n).astype(BF16)
    out[:, :capacity, :] = dot(pick, own).astype(BF16).reshape(experts, capacity, narrow)
    half = gate.shape[2]
    gains[...] = jnp.broadcast_to(column(gain[...]), gains.shape)
    at = pl.multiple_of(lax.axis_index("grp") * piece, TILE)
    g = gains[pl.ds(at, piece), :][None]
    out[:, capacity:, :half] = (gate[:, pl.ds(at, piece), :] * g).astype(BF16)
    out[:, capacity:, half:] = (up[:, pl.ds(at, piece), :] * g).astype(BF16)


def expert_kernel(*refs, parts, cores):
    gate, up, hidden, mixed = refs[-4:]
    weights, slices = refs[:parts], refs[parts:-4]
    half = gate.shape[2]
    total = len(slices)
    narrow = slices[0].shape[1]

    @pl.when(pl.program_id(0) == 0)
    def _():
        piece = weights[0].shape[2]
        mine = lax.axis_index("grp")
        q = 0
        for ref in weights:
            for j in range(ref.shape[0]):
                at = pl.multiple_of((mine ^ q) * piece, TILE)
                gate[:, pl.ds(at, piece), :] = ref[j, :, :, :half]
                up[:, pl.ds(at, piece), :] = ref[j, :, :, half:]
                q += 1
        tp = lax.axis_index("tp")
        per = gate.shape[0] // total
        for k, where in enumerate(slice_places(total, cores)):
            at = where(tp) * per
            mixed[k, :, :half] = gate[pl.ds(at, per)].reshape(narrow, half)
            mixed[k, :, half:] = up[pl.ds(at, per)].reshape(narrow, half)

    a = dot(slices[0][...], mixed[0])
    for k in range(1, total):
        a = a + dot(slices[k][...], mixed[k])
    g = a[:, :half]
    hidden[...] = (g / (1.0 + jnp.exp(-g)) * a[:, half:]).astype(BF16)


def place_kernel(chosen, affinity, take, share, *, experts, capacity):
    top, n = chosen.shape
    lines, total = take.shape
    choice = chosen[...].astype(F32)
    _, slot = slots_of(choice, experts)
    expert = iota((experts, n), 0).astype(F32)
    a = affinity[...]
    part = a / jnp.sum(a, axis=0, keepdims=True)
    line = iota((lines, n), 0)
    here = line // top == iota((lines, n), 1)
    at = jnp.zeros((lines, n), F32)
    of = jnp.zeros((lines, n), F32)
    for k in range(top):
        c = choice[k : k + 1, :]
        goal = jnp.sum(jnp.where(c == expert, slot, 0.0), axis=0, keepdims=True) + c * capacity
        this = here & (line % top == k)
        at = jnp.where(this, goal, at)
        of = jnp.where(this, part[k : k + 1, :], of)
    at = jnp.sum(at, axis=1, keepdims=True)
    take[...] = (iota((lines, total), 1).astype(F32) == at).astype(F32).astype(BF16)
    share[...] = jnp.broadcast_to(jnp.sum(of, axis=1, keepdims=True), share.shape)


def pick_kernel(back, take, share, out):
    out[...] = (dot(take[...], back[...]) * share[...]).astype(BF16)


def ring_tables(total, cores):
    def hop(sign):
        def to(i):
            turn = sign if i % cores == 0 else -sign
            return (i + turn * cores) % total

        return [(i, to(i)) for i in range(total)]

    return hop(1), hop(-1), [(i, i ^ 1) for i in range(total)]


def slice_places(total, cores):
    chips = total // cores

    def away(steps):
        def place(i):
            turn = jnp.where(i % cores == 0, -steps, steps)
            return (i + turn * cores + total) % total

        return place

    places = [away(0)]
    for s in range(1, chips // 2 + 1):
        places.append(away(s))
        if s <= (chips - 1) // 2:
            places.append(away(-s))
    return places + [lambda i, p=p: p(i ^ 1) for p in places]


def gather_slices(own, total, cores):
    ahead, behind, swap = ring_tables(total, cores)
    chips = total // cores
    got = [own]
    one = two = own
    for s in range(1, chips // 2 + 1):
        one = lax.ppermute(one, "tp", ahead)
        got.append(one)
        if s <= (chips - 1) // 2:
            two = lax.ppermute(two, "tp", behind)
            got.append(two)
    return got + [lax.ppermute(g, "tp", swap) for g in got]


def gather_groups(own, groups):
    got = [own]
    step = 1
    while step < groups:
        send = got[0] if len(got) == 1 else jnp.concatenate(got, axis=0)
        table = [(i, i ^ step) for i in range(groups)]
        got.append(lax.ppermute(send, "grp", table))
        step *= 2
    return got


def on_device(tokens, norm_gain, gate_master, up_master, chosen, affinity):
    groups, sources, total = (lax.axis_size(a) for a in ("grp", "fs", "tp"))
    experts, block, half = gate_master.shape
    n, width = tokens.shape
    top = chosen.shape[1]
    capacity = n * top * 2 // experts
    narrow = width // total
    piece = block // groups
    vmem = pl.BlockSpec(memory_space=pltpu.VMEM)

    sent = pl.pallas_call(
        functools.partial(
            pack_kernel, experts=experts, capacity=capacity, narrow=narrow, piece=piece
        ),
        out_shape=jax.ShapeDtypeStruct((experts, capacity + piece, narrow), BF16),
        in_specs=[vmem] * 5,
        out_specs=vmem,
        scratch_shapes=[pltpu.VMEM((block, half), F32)],
        name="pack",
    )(tokens, chosen.T, norm_gain[None, :], gate_master, up_master)
    got = lax.all_to_all(sent, "fs", split_axis=0, concat_axis=0, tiled=True)
    rows = got[:, :capacity, :].reshape(sources * capacity, narrow)
    weights = gather_groups(got[None, :, capacity:, :], groups)
    slices = gather_slices(rows, total, CORES)

    slots = sources * capacity
    rows_at = lambda i: (i, 0)
    fixed = lambda dims: pl.BlockSpec(dims, lambda i: (0,) * len(dims))
    gate, up, hidden = pl.pallas_call(
        functools.partial(expert_kernel, parts=len(weights), cores=CORES),
        grid=(STEPS,),
        out_shape=(
            jax.ShapeDtypeStruct((sources, block, half), BF16),
            jax.ShapeDtypeStruct((sources, block, half), BF16),
            jax.ShapeDtypeStruct((slots, half), BF16),
        ),
        in_specs=[fixed(w.shape) for w in weights]
        + [pl.BlockSpec((slots // STEPS, narrow), rows_at) for _ in slices],
        out_specs=(
            fixed((sources, block, half)),
            fixed((sources, block, half)),
            pl.BlockSpec((slots // STEPS, half), rows_at),
        ),
        scratch_shapes=[pltpu.VMEM((total, narrow, 2 * half), BF16)],
        name="experts",
    )(*weights, *slices)
    hidden, choice, ratio = lax.optimization_barrier((hidden, chosen.T, affinity.T))
    back = lax.all_to_all(
        hidden.reshape(sources, capacity, half), "fs", split_axis=0, concat_axis=0, tiled=True
    )
    take, share = pl.pallas_call(
        functools.partial(place_kernel, experts=experts, capacity=capacity),
        out_shape=(
            jax.ShapeDtypeStruct((n * top, experts * capacity), BF16),
            jax.ShapeDtypeStruct((n * top, half), F32),
        ),
        in_specs=[vmem] * 2,
        out_specs=(vmem, vmem),
        name="place",
    )(choice, ratio)
    out = pl.pallas_call(
        pick_kernel,
        out_shape=jax.ShapeDtypeStruct((n * top, half), BF16),
        in_specs=[vmem] * 3,
        out_specs=vmem,
        name="pick",
    )(back.reshape(experts * capacity, half), take, share)
    return (
        gate.reshape(1, sources * block, half),
        up.reshape(1, sources * block, half),
        out.reshape(n, top, half),
    )


def solution(mesh):
    return jax.shard_map(
        on_device,
        mesh=mesh,
        in_specs=(
            P(("grp", "fs"), None),
            P("fs"),
            P(None, "fs", "tp"),
            P(None, "fs", "tp"),
            P(("grp", "fs"), None),
            P(("grp", "fs"), None),
        ),
        out_specs=(
            P(("grp", "fs"), None, "tp"),
            P(("grp", "fs"), None, "tp"),
            P(("grp", "fs"), None, "tp"),
        ),
        check_vma=False,
    )
```

```python
import functools
import jax
import jax.numpy as jnp
from jax import lax
from jax.experimental import pallas as pl
from jax.experimental.pallas import tpu as pltpu
from jax.sharding import PartitionSpec as P

F32 = jnp.float32
BF16 = jnp.bfloat16
CORES = 2
TILE = 8
PARAMS = pltpu.CompilerParams(vmem_limit_bytes=16 << 20)


def iota(shape, dim):
    return lax.broadcasted_iota(jnp.int32, shape, dim)


def dot(a, b, dims=(((1,), (0,)), ((), ()))):
    return lax.dot_general(a, b, dims, preferred_element_type=F32)


def column(row):
    n = row.shape[1]
    return jnp.sum(jnp.where(iota((n, n), 0) == iota((n, n), 1), row, 0.0), axis=1, keepdims=True)


def slots_of(choice, experts):
    top, n = choice.shape
    expert = iota((experts, n), 0).astype(F32)
    named = jnp.zeros((experts, n), F32)
    for k in range(top):
        named = named + (choice[k : k + 1, :] == expert).astype(F32)
    before = (iota((n, n), 0) < iota((n, n), 1)).astype(F32).astype(BF16)
    return named, dot(named.astype(BF16), before)


def pack_kernel(tokens, chosen, gain, gate, up, out, gains, *, experts, capacity, narrow, piece):
    n, width = tokens.shape
    x = tokens[...].astype(F32)
    scale = lax.rsqrt(jnp.sum(x * x, axis=-1, keepdims=True) / width + 1e-06)
    at = pl.multiple_of(lax.axis_index("tp") * narrow, narrow)
    own = (tokens[:, pl.ds(at, narrow)].astype(F32) * scale).astype(BF16)
    named, slot = slots_of(chosen[...].astype(F32), experts)
    slot = jnp.where(named > 0, slot, -1.0)
    pick = slot[:, None, :] == iota((experts, capacity, n), 1).astype(F32)
    pick = pick.astype(F32).reshape(experts * capacity, n).astype(BF16)
    out[:, :capacity, :] = dot(pick, own).astype(BF16).reshape(experts, capacity, narrow)
    half = gate.shape[2]
    gains[...] = jnp.broadcast_to(column(gain[...]), gains.shape)
    at = pl.multiple_of(lax.axis_index("grp") * piece, TILE)
    g = gains[pl.ds(at, piece), :][None]
    out[:, capacity:, :half] = (gate[:, pl.ds(at, piece), :] * g).astype(BF16)
    out[:, capacity:, half:] = (up[:, pl.ds(at, piece), :] * g).astype(BF16)


def expert_kernel(*refs, parts, cores):
    gate, up, hidden, mixed = refs[-4:]
    weights, slices = refs[:parts], refs[parts:-4]
    half = gate.shape[2]
    total = len(slices)
    narrow = slices[0].shape[1]

    piece = weights[0].shape[2]
    mine = lax.axis_index("grp")
    q = 0
    for ref in weights:
        for j in range(ref.shape[0]):
            at = pl.multiple_of((mine ^ q) * piece, TILE)
            gate[:, pl.ds(at, piece), :] = ref[j, :, :, :half]
            up[:, pl.ds(at, piece), :] = ref[j, :, :, half:]
            q += 1
    tp = lax.axis_index("tp")
    per = gate.shape[0] // total
    for k, where in enumerate(slice_places(total, cores)):
        at = where(tp) * per
        mixed[k, :, :half] = gate[pl.ds(at, per)].reshape(narrow, half)
        mixed[k, :, half:] = up[pl.ds(at, per)].reshape(narrow, half)
    a = dot(slices[0][...], mixed[0])
    for k in range(1, total):
        a = a + dot(slices[k][...], mixed[k])
    g = a[:, :half]
    hidden[...] = (g / (1.0 + jnp.exp(-g)) * a[:, half:]).astype(BF16)


def place_kernel(chosen, affinity, take, share, *, experts, capacity):
    top, n = chosen.shape
    lines, total = take.shape
    choice = chosen[...].astype(F32)
    _, slot = slots_of(choice, experts)
    expert = iota((experts, n), 0).astype(F32)
    a = affinity[...]
    part = a / jnp.sum(a, axis=0, keepdims=True)
    line = iota((lines, n), 0)
    here = line // top == iota((lines, n), 1)
    at = jnp.zeros((lines, n), F32)
    of = jnp.zeros((lines, n), F32)
    for k in range(top):
        c = choice[k : k + 1, :]
        goal = jnp.sum(jnp.where(c == expert, slot, 0.0), axis=0, keepdims=True) + c * capacity
        this = here & (line % top == k)
        at = jnp.where(this, goal, at)
        of = jnp.where(this, part[k : k + 1, :], of)
    at = jnp.sum(at, axis=1, keepdims=True)
    take[...] = (iota((lines, total), 1).astype(F32) == at).astype(F32).astype(BF16)
    share[...] = jnp.broadcast_to(jnp.sum(of, axis=1, keepdims=True), share.shape)


def pick_kernel(back, take, share, out):
    out[...] = (dot(take[...], back[...]) * share[...]).astype(BF16)


def ring_tables(total, cores):
    def hop(sign):
        def to(i):
            turn = sign if i % cores == 0 else -sign
            return (i + turn * cores) % total

        return [(i, to(i)) for i in range(total)]

    return hop(1), hop(-1), [(i, i ^ 1) for i in range(total)]


def slice_places(total, cores):
    chips = total // cores

    def away(steps):
        def place(i):
            turn = jnp.where(i % cores == 0, -steps, steps)
            return (i + turn * cores + total) % total

        return place

    places = [away(0)]
    for s in range(1, chips // 2 + 1):
        places.append(away(s))
        if s <= (chips - 1) // 2:
            places.append(away(-s))
    return places + [lambda i, p=p: p(i ^ 1) for p in places]


def gather_slices(own, total, cores):
    ahead, behind, swap = ring_tables(total, cores)
    chips = total // cores
    got = [own]
    one = two = own
    for s in range(1, chips // 2 + 1):
        one = lax.ppermute(one, "tp", ahead)
        got.append(one)
        if s <= (chips - 1) // 2:
            two = lax.ppermute(two, "tp", behind)
            got.append(two)
    return got + [lax.ppermute(g, "tp", swap) for g in got]


def gather_groups(own, groups):
    got = [own]
    step = 1
    while step < groups:
        send = got[0] if len(got) == 1 else jnp.concatenate(got, axis=0)
        table = [(i, i ^ step) for i in range(groups)]
        got.append(lax.ppermute(send, "grp", table))
        step *= 2
    return got


def on_device(tokens, norm_gain, gate_master, up_master, chosen, affinity):
    groups, sources, total = (lax.axis_size(a) for a in ("grp", "fs", "tp"))
    experts, block, half = gate_master.shape
    n, width = tokens.shape
    top = chosen.shape[1]
    capacity = n * top * 2 // experts
    narrow = width // total
    piece = block // groups
    vmem = pl.BlockSpec(memory_space=pltpu.VMEM)

    sent = pl.pallas_call(
        functools.partial(
            pack_kernel, experts=experts, capacity=capacity, narrow=narrow, piece=piece
        ),
        out_shape=jax.ShapeDtypeStruct((experts, capacity + piece, narrow), BF16),
        in_specs=[vmem] * 5,
        out_specs=vmem,
        scratch_shapes=[pltpu.VMEM((block, half), F32)],
        compiler_params=PARAMS,
        name="pack",
    )(tokens, chosen.T, norm_gain[None, :], gate_master, up_master)
    got = lax.all_to_all(sent, "fs", split_axis=0, concat_axis=0, tiled=True)
    rows = got[:, :capacity, :].reshape(sources * capacity, narrow)
    weights = gather_groups(got[None, :, capacity:, :], groups)
    slices = gather_slices(rows, total, CORES)

    gate, up, hidden = pl.pallas_call(
        functools.partial(expert_kernel, parts=len(weights), cores=CORES),
        out_shape=(
            jax.ShapeDtypeStruct((sources, block, half), BF16),
            jax.ShapeDtypeStruct((sources, block, half), BF16),
            jax.ShapeDtypeStruct((sources * capacity, half), BF16),
        ),
        in_specs=[vmem] * (len(weights) + len(slices)),
        out_specs=(vmem, vmem, vmem),
        scratch_shapes=[pltpu.VMEM((total, narrow, 2 * half), BF16)],
        compiler_params=PARAMS,
        name="experts",
    )(*weights, *slices)
    hidden, choice, ratio = lax.optimization_barrier((hidden, chosen.T, affinity.T))
    back = lax.all_to_all(
        hidden.reshape(sources, capacity, half), "fs", split_axis=0, concat_axis=0, tiled=True
    )
    take, share = pl.pallas_call(
        functools.partial(place_kernel, experts=experts, capacity=capacity),
        out_shape=(
            jax.ShapeDtypeStruct((n * top, experts * capacity), BF16),
            jax.ShapeDtypeStruct((n * top, half), F32),
        ),
        in_specs=[vmem] * 2,
        out_specs=(vmem, vmem),
        compiler_params=PARAMS,
        name="place",
    )(choice, ratio)
    out = pl.pallas_call(
        pick_kernel,
        out_shape=jax.ShapeDtypeStruct((n * top, half), BF16),
        in_specs=[vmem] * 3,
        out_specs=vmem,
        compiler_params=PARAMS,
        name="pick",
    )(back.reshape(experts * capacity, half), take, share)
    return (
        gate.reshape(1, sources * block, half),
        up.reshape(1, sources * block, half),
        out.reshape(n, top, half),
    )


def solution(mesh):
    return jax.shard_map(
        on_device,
        mesh=mesh,
        in_specs=(
            P(("grp", "fs"), None),
            P("fs"),
            P(None, "fs", "tp"),
            P(None, "fs", "tp"),
            P(("grp", "fs"), None),
            P(("grp", "fs"), None),
        ),
        out_specs=(
            P(("grp", "fs"), None, "tp"),
            P(("grp", "fs"), None, "tp"),
            P(("grp", "fs"), None, "tp"),
        ),
        check_vma=False,
    )
```

```python
import functools
import jax
import jax.numpy as jnp
from jax import lax
from jax.experimental import pallas as pl
from jax.experimental.pallas import tpu as pltpu
from jax.sharding import PartitionSpec as P

F32 = jnp.float32
BF16 = jnp.bfloat16
CORES = 2
TILE = 8
PARTS = 4
PARAMS = pltpu.CompilerParams(vmem_limit_bytes=16 << 20)


def iota(shape, dim):
    return lax.broadcasted_iota(jnp.int32, shape, dim)


def dot(a, b, dims=(((1,), (0,)), ((), ()))):
    return lax.dot_general(a, b, dims, preferred_element_type=F32)


def column(row):
    n = row.shape[1]
    return jnp.sum(jnp.where(iota((n, n), 0) == iota((n, n), 1), row, 0.0), axis=1, keepdims=True)


def slots_of(choice, experts):
    top, n = choice.shape
    expert = iota((experts, n), 0).astype(F32)
    named = jnp.zeros((experts, n), F32)
    for k in range(top):
        named = named + (choice[k : k + 1, :] == expert).astype(F32)
    before = (iota((n, n), 0) < iota((n, n), 1)).astype(F32).astype(BF16)
    return named, dot(named.astype(BF16), before)


def pack_kernel(
    tokens, chosen, gain, gate, up, out, tok, cho, gai, gat, upp, gains, sems, *, experts, capacity
):
    n, width = tok.shape
    narrow = out.shape[2]
    piece, half = gat.shape[1:]
    part = n // PARTS
    mine = pl.multiple_of(lax.axis_index("grp") * piece, TILE)
    pairs = [(chosen, cho), (gain, gai)]
    pairs += [(tokens.at[pl.ds(i * part, part)], tok.at[pl.ds(i * part, part)]) for i in range(PARTS)]
    pairs += [(gate.at[:, pl.ds(mine, piece), :], gat), (up.at[:, pl.ds(mine, piece), :], upp)]
    copies = [pltpu.make_async_copy(a, b, sems.at[i]) for i, (a, b) in enumerate(pairs)]
    for c in copies:
        c.start()
    copies[0].wait()
    named, slot = slots_of(cho[...].astype(F32), experts)
    slot = jnp.where(named > 0, slot, -1.0)
    pick = slot[:, None, :] == iota((experts, capacity, n), 1).astype(F32)
    pick = pick.astype(F32).reshape(experts * capacity, n).astype(BF16)
    copies[1].wait()
    gains[...] = jnp.broadcast_to(column(gai[...]), gains.shape)
    for c in copies[2 : 2 + PARTS]:
        c.wait()
    x = tok[...].astype(F32)
    scale = lax.rsqrt(jnp.sum(x * x, axis=-1, keepdims=True) / width + 1e-06)
    at = pl.multiple_of(lax.axis_index("tp") * narrow, narrow)
    own = (tok[:, pl.ds(at, narrow)].astype(F32) * scale).astype(BF16)
    out[:, :capacity, :] = dot(pick, own).astype(BF16).reshape(experts, capacity, narrow)
    for c in copies[2 + PARTS :]:
        c.wait()
    g = gains[pl.ds(mine, piece), :][None]
    out[:, capacity:, :half] = (gat[...] * g).astype(BF16)
    out[:, capacity:, half:] = (upp[...] * g).astype(BF16)


def expert_kernel(*refs, parts, cores):
    gate, up, hidden, mixed = refs[-4:]
    weights, slices = refs[:parts], refs[parts:-4]
    half = gate.shape[2]
    total = len(slices)
    narrow = slices[0].shape[1]

    piece = weights[0].shape[2]
    mine = lax.axis_index("grp")
    q = 0
    for ref in weights:
        for j in range(ref.shape[0]):
            at = pl.multiple_of((mine ^ q) * piece, TILE)
            gate[:, pl.ds(at, piece), :] = ref[j, :, :, :half]
            up[:, pl.ds(at, piece), :] = ref[j, :, :, half:]
            q += 1
    tp = lax.axis_index("tp")
    per = gate.shape[0] // total
    for k, where in enumerate(slice_places(total, cores)):
        at = where(tp) * per
        mixed[k, :, :half] = gate[pl.ds(at, per)].reshape(narrow, half)
        mixed[k, :, half:] = up[pl.ds(at, per)].reshape(narrow, half)
    a = dot(slices[0][...], mixed[0])
    for k in range(1, total):
        a = a + dot(slices[k][...], mixed[k])
    g = a[:, :half]
    hidden[...] = (g / (1.0 + jnp.exp(-g)) * a[:, half:]).astype(BF16)


def place_kernel(chosen, affinity, take, share, *, experts, capacity):
    top, n = chosen.shape
    lines, total = take.shape
    choice = chosen[...].astype(F32)
    _, slot = slots_of(choice, experts)
    expert = iota((experts, n), 0).astype(F32)
    a = affinity[...]
    part = a / jnp.sum(a, axis=0, keepdims=True)
    line = iota((lines, n), 0)
    here = line // top == iota((lines, n), 1)
    at = jnp.zeros((lines, n), F32)
    of = jnp.zeros((lines, n), F32)
    for k in range(top):
        c = choice[k : k + 1, :]
        goal = jnp.sum(jnp.where(c == expert, slot, 0.0), axis=0, keepdims=True) + c * capacity
        this = here & (line % top == k)
        at = jnp.where(this, goal, at)
        of = jnp.where(this, part[k : k + 1, :], of)
    at = jnp.sum(at, axis=1, keepdims=True)
    take[...] = (iota((lines, total), 1).astype(F32) == at).astype(F32).astype(BF16)
    share[...] = jnp.broadcast_to(jnp.sum(of, axis=1, keepdims=True), share.shape)


def pick_kernel(back, take, share, out):
    out[...] = (dot(take[...], back[...]) * share[...]).astype(BF16)


def ring_tables(total, cores):
    def hop(sign):
        def to(i):
            turn = sign if i % cores == 0 else -sign
            return (i + turn * cores) % total

        return [(i, to(i)) for i in range(total)]

    return hop(1), hop(-1), [(i, i ^ 1) for i in range(total)]


def slice_places(total, cores):
    chips = total // cores

    def away(steps):
        def place(i):
            turn = jnp.where(i % cores == 0, -steps, steps)
            return (i + turn * cores + total) % total

        return place

    places = [away(0)]
    for s in range(1, chips // 2 + 1):
        places.append(away(s))
        if s <= (chips - 1) // 2:
            places.append(away(-s))
    return places + [lambda i, p=p: p(i ^ 1) for p in places]


def gather_slices(own, total, cores):
    ahead, behind, swap = ring_tables(total, cores)
    chips = total // cores
    got = [own]
    one = two = own
    for s in range(1, chips // 2 + 1):
        one = lax.ppermute(one, "tp", ahead)
        got.append(one)
        if s <= (chips - 1) // 2:
            two = lax.ppermute(two, "tp", behind)
            got.append(two)
    return got + [lax.ppermute(g, "tp", swap) for g in got]


def gather_groups(own, groups):
    got = [own]
    step = 1
    while step < groups:
        send = got[0] if len(got) == 1 else jnp.concatenate(got, axis=0)
        table = [(i, i ^ step) for i in range(groups)]
        got.append(lax.ppermute(send, "grp", table))
        step *= 2
    return got


def on_device(tokens, norm_gain, gate_master, up_master, chosen, affinity):
    groups, sources, total = (lax.axis_size(a) for a in ("grp", "fs", "tp"))
    experts, block, half = gate_master.shape
    n, width = tokens.shape
    top = chosen.shape[1]
    capacity = n * top * 2 // experts
    narrow = width // total
    piece = block // groups
    vmem = pl.BlockSpec(memory_space=pltpu.VMEM)

    sent = pl.pallas_call(
        functools.partial(pack_kernel, experts=experts, capacity=capacity),
        out_shape=jax.ShapeDtypeStruct((experts, capacity + piece, narrow), BF16),
        in_specs=[pl.BlockSpec(memory_space=pltpu.HBM)] * 5,
        out_specs=vmem,
        scratch_shapes=[
            pltpu.VMEM((n, width), BF16),
            pltpu.VMEM((top, n), jnp.int32),
            pltpu.VMEM((1, block), F32),
            pltpu.VMEM((experts, piece, half), F32),
            pltpu.VMEM((experts, piece, half), F32),
            pltpu.VMEM((block, half), F32),
            pltpu.SemaphoreType.DMA((PARTS + 4,)),
        ],
        compiler_params=PARAMS,
        name="pack",
    )(*(
        pltpu.with_memory_space_constraint(a, pltpu.HBM)
        for a in (tokens, chosen.T, norm_gain[None, :], gate_master, up_master)
    ))
    got = lax.all_to_all(sent, "fs", split_axis=0, concat_axis=0, tiled=True)
    rows = got[:, :capacity, :].reshape(sources * capacity, narrow)
    weights = gather_groups(got[None, :, capacity:, :], groups)
    slices = gather_slices(rows, total, CORES)

    gate, up, hidden = pl.pallas_call(
        functools.partial(expert_kernel, parts=len(weights), cores=CORES),
        out_shape=(
            jax.ShapeDtypeStruct((sources, block, half), BF16),
            jax.ShapeDtypeStruct((sources, block, half), BF16),
            jax.ShapeDtypeStruct((sources * capacity, half), BF16),
        ),
        in_specs=[vmem] * (len(weights) + len(slices)),
        out_specs=(vmem, vmem, vmem),
        scratch_shapes=[pltpu.VMEM((total, narrow, 2 * half), BF16)],
        compiler_params=PARAMS,
        name="experts",
    )(*weights, *slices)
    hidden, choice, ratio = lax.optimization_barrier((hidden, chosen.T, affinity.T))
    back = lax.all_to_all(
        hidden.reshape(sources, capacity, half), "fs", split_axis=0, concat_axis=0, tiled=True
    )
    take, share = pl.pallas_call(
        functools.partial(place_kernel, experts=experts, capacity=capacity),
        out_shape=(
            jax.ShapeDtypeStruct((n * top, experts * capacity), BF16),
            jax.ShapeDtypeStruct((n * top, half), F32),
        ),
        in_specs=[vmem] * 2,
        out_specs=(vmem, vmem),
        compiler_params=PARAMS,
        name="place",
    )(choice, ratio)
    out = pl.pallas_call(
        pick_kernel,
        out_shape=jax.ShapeDtypeStruct((n * top, half), BF16),
        in_specs=[vmem] * 3,
        out_specs=vmem,
        compiler_params=PARAMS,
        name="pick",
    )(back.reshape(experts * capacity, half), take, share)
    return (
        gate.reshape(1, sources * block, half),
        up.reshape(1, sources * block, half),
        out.reshape(n, top, half),
    )


def solution(mesh):
    return jax.shard_map(
        on_device,
        mesh=mesh,
        in_specs=(
            P(("grp", "fs"), None),
            P("fs"),
            P(None, "fs", "tp"),
            P(None, "fs", "tp"),
            P(("grp", "fs"), None),
            P(("grp", "fs"), None),
        ),
        out_specs=(
            P(("grp", "fs"), None, "tp"),
            P(("grp", "fs"), None, "tp"),
            P(("grp", "fs"), None, "tp"),
        ),
        check_vma=False,
    )
```

```python
import functools
import jax
import jax.numpy as jnp
from jax import lax
from jax.experimental import pallas as pl
from jax.experimental.pallas import tpu as pltpu
from jax.sharding import PartitionSpec as P

F32 = jnp.float32
BF16 = jnp.bfloat16
CORES = 2
TILE = 8
PARTS = 4
PARAMS = pltpu.CompilerParams(vmem_limit_bytes=16 << 20)


def iota(shape, dim):
    return lax.broadcasted_iota(jnp.int32, shape, dim)


def dot(a, b, dims=(((1,), (0,)), ((), ()))):
    return lax.dot_general(a, b, dims, preferred_element_type=F32)


def column(row):
    n = row.shape[1]
    return jnp.sum(jnp.where(iota((n, n), 0) == iota((n, n), 1), row, 0.0), axis=1, keepdims=True)


def slots_of(choice, experts):
    top, n = choice.shape
    expert = iota((experts, n), 0).astype(F32)
    named = jnp.zeros((experts, n), F32)
    for k in range(top):
        named = named + (choice[k : k + 1, :] == expert).astype(F32)
    before = (iota((n, n), 0) < iota((n, n), 1)).astype(F32).astype(BF16)
    return named, dot(named.astype(BF16), before)


def pack_kernel(
    tokens, chosen, gain, gate, up, out, tok, cho, gai, gat, upp, gains, sems, *, experts, capacity
):
    n, width = tok.shape
    narrow = out.shape[2]
    piece, half = gat.shape[1:]
    share = capacity // CORES
    part = n // PARTS
    mine = pl.multiple_of(lax.axis_index("grp") * piece, TILE)
    pairs = [(chosen, cho), (gain, gai)]
    pairs += [(tokens.at[pl.ds(i * part, part)], tok.at[pl.ds(i * part, part)]) for i in range(PARTS)]
    pairs += [(gate.at[:, pl.ds(mine, piece), :], gat), (up.at[:, pl.ds(mine, piece), :], upp)]
    copies = [pltpu.make_async_copy(a, b, sems.at[i]) for i, (a, b) in enumerate(pairs)]
    for c in copies:
        c.start()
    copies[0].wait()
    named, slot = slots_of(cho[...].astype(F32), experts)
    slot = jnp.where(named > 0, slot, -1.0)
    first = lax.axis_index("core") * share
    pick = slot[:, None, :] == (iota((experts, share, n), 1) + first).astype(F32)
    pick = pick.astype(F32).reshape(experts * share, n).astype(BF16)
    copies[1].wait()
    gains[...] = jnp.broadcast_to(column(gai[...]), gains.shape)
    for c in copies[2 : 2 + PARTS]:
        c.wait()
    x = tok[...].astype(F32)
    scale = lax.rsqrt(jnp.sum(x * x, axis=-1, keepdims=True) / width + 1e-06)
    for c in range(CORES):
        at = pl.multiple_of((lax.axis_index("x") * CORES + c) * narrow, narrow)
        own = (tok[:, pl.ds(at, narrow)].astype(F32) * scale).astype(BF16)
        rows = dot(pick, own).astype(BF16).reshape(experts, share, narrow)
        out[:, c * share : (c + 1) * share, :] = rows
    for c in copies[2 + PARTS :]:
        c.wait()
    g = gains[pl.ds(mine, piece), :][None]
    out[:, capacity:, :half] = (gat[...] * g).astype(BF16)
    out[:, capacity:, half:] = (upp[...] * g).astype(BF16)


def expert_kernel(*refs, parts, chips):
    gate, up, hidden, mixed = refs[-4:]
    weights, others, slices = refs[:parts], refs[parts : 2 * parts], refs[2 * parts : -4]
    half = gate.shape[2]
    block = gate.shape[1]
    slots, narrow = slices[0].shape[1:]
    share = slots // CORES
    total = chips * CORES
    per = gate.shape[0] // total
    piece = weights[0].shape[2]
    mine = lax.axis_index("grp")
    x = lax.axis_index("x")
    core = lax.axis_index("core")
    chip = [place(x, core, chips) for place in chip_places(chips)]
    for side, group in enumerate((weights, others)):
        q = 0
        for ref in group:
            for j in range(ref.shape[0]):
                at = pl.multiple_of((mine ^ q) * piece, TILE)
                if side == 0:
                    gate[:, pl.ds(at, piece), :] = ref[j, :, :, :half]
                    up[:, pl.ds(at, piece), :] = ref[j, :, :, half:]
                for i, c in enumerate(chip):
                    part = ref[j, pl.ds(c * CORES * per, CORES * per)]
                    mixed[i, :, pl.ds(at, piece), side * narrow : (side + 1) * narrow] = part
                q += 1
    a = None
    for i, ref in enumerate(slices):
        for c in range(CORES):
            rows = ref[:, c * share : (c + 1) * share, :].reshape(-1, narrow)
            w = mixed[i, c * per : (c + 1) * per].reshape(per * block, CORES * narrow)
            d = dot(rows, w)
            a = d if a is None else a + d
    for side, to in enumerate((core, 1 - core)):
        g = a[:, side * narrow : side * narrow + half]
        u = a[:, side * narrow + half : (side + 1) * narrow]
        h = (g / (1.0 + jnp.exp(-g)) * u).astype(BF16)
        hidden[:, pl.ds(to, 1)] = h.reshape(hidden.shape[0], 1, share, half)


def place_kernel(chosen, affinity, take, share, *, experts, capacity):
    top, n = chosen.shape
    lines, total = take.shape
    choice = chosen[...].astype(F32)
    _, slot = slots_of(choice, experts)
    expert = iota((experts, n), 0).astype(F32)
    a = affinity[...]
    part = a / jnp.sum(a, axis=0, keepdims=True)
    line = iota((lines, n), 0)
    here = line // top == iota((lines, n), 1)
    at = jnp.zeros((lines, n), F32)
    of = jnp.zeros((lines, n), F32)
    for k in range(top):
        c = choice[k : k + 1, :]
        goal = jnp.sum(jnp.where(c == expert, slot, 0.0), axis=0, keepdims=True) + c * capacity
        this = here & (line % top == k)
        at = jnp.where(this, goal, at)
        of = jnp.where(this, part[k : k + 1, :], of)
    at = jnp.sum(at, axis=1, keepdims=True)
    take[...] = (iota((lines, total), 1).astype(F32) == at).astype(F32).astype(BF16)
    share[...] = jnp.broadcast_to(jnp.sum(of, axis=1, keepdims=True), share.shape)


def pick_kernel(back, take, share, out):
    out[...] = (dot(take[...], back[...]) * share[...]).astype(BF16)


def chip_places(chips):
    def away(steps):
        return lambda x, core, n: (x + jnp.where(core == 0, -steps, steps) + n) % n

    places = [away(0)]
    for s in range(1, chips // 2 + 1):
        places.append(away(s))
        if s <= (chips - 1) // 2:
            places.append(away(-s))
    return places


def gather_slices(own, chips):
    def hop(sign):
        def to(x, c):
            return (x + (sign if c == 0 else -sign)) % chips

        pairs = [(x, c) for x in range(chips) for c in range(CORES)]
        return [(x * CORES + c, to(x, c) * CORES + c) for x, c in pairs]

    got = [own]
    one = two = own
    for s in range(1, chips // 2 + 1):
        one = lax.ppermute(one, ("x", "core"), hop(1))
        got.append(one)
        if s <= (chips - 1) // 2:
            two = lax.ppermute(two, ("x", "core"), hop(-1))
            got.append(two)
    return got


def gather_groups(own, groups):
    got = [own]
    step = 1
    while step < groups:
        send = got[0] if len(got) == 1 else jnp.concatenate(got, axis=0)
        table = [(i, i ^ step) for i in range(groups)]
        got.append(lax.ppermute(send, "grp", table))
        step *= 2
    return got


def on_device(tokens, norm_gain, gate_master, up_master, chosen, affinity):
    groups, sources, chips = (lax.axis_size(a) for a in ("grp", "fs", "x"))
    total = chips * CORES
    experts, block, half = gate_master.shape
    n, width = tokens.shape
    top = chosen.shape[1]
    capacity = n * top * 2 // experts
    narrow = width // total
    piece = block // groups
    vmem = pl.BlockSpec(memory_space=pltpu.VMEM)

    sent = pl.pallas_call(
        functools.partial(pack_kernel, experts=experts, capacity=capacity),
        out_shape=jax.ShapeDtypeStruct((experts, capacity + piece, narrow), BF16),
        in_specs=[pl.BlockSpec(memory_space=pltpu.HBM)] * 5,
        out_specs=vmem,
        scratch_shapes=[
            pltpu.VMEM((n, width), BF16),
            pltpu.VMEM((top, n), jnp.int32),
            pltpu.VMEM((1, block), F32),
            pltpu.VMEM((experts, piece, half), F32),
            pltpu.VMEM((experts, piece, half), F32),
            pltpu.VMEM((block, half), F32),
            pltpu.SemaphoreType.DMA((PARTS + 4,)),
        ],
        compiler_params=PARAMS,
        name="pack",
    )(*(
        pltpu.with_memory_space_constraint(a, pltpu.HBM)
        for a in (tokens, chosen.T, norm_gain[None, :], gate_master, up_master)
    ))
    got = lax.all_to_all(sent, "fs", split_axis=0, concat_axis=0, tiled=True)
    rows = got[:, :capacity, :]
    weights = gather_groups(got[None, :, capacity:, :], groups)
    slices = gather_slices(rows, chips)
    swap = [(c, 1 - c) for c in range(CORES)]
    others = [lax.ppermute(w, "core", swap) for w in weights]
    share = capacity // CORES

    gate, up, hidden = pl.pallas_call(
        functools.partial(expert_kernel, parts=len(weights), chips=chips),
        out_shape=(
            jax.ShapeDtypeStruct((sources, block, half), BF16),
            jax.ShapeDtypeStruct((sources, block, half), BF16),
            jax.ShapeDtypeStruct((sources, CORES, share, half), BF16),
        ),
        in_specs=[vmem] * (2 * len(weights) + len(slices)),
        out_specs=(vmem, vmem, vmem),
        scratch_shapes=[pltpu.VMEM((chips, CORES * sources // total, block, CORES * narrow), BF16)],
        compiler_params=PARAMS,
        name="experts",
    )(*weights, *others, *slices)
    hidden, choice, ratio = lax.optimization_barrier((hidden, chosen.T, affinity.T))
    back = lax.all_to_all(
        hidden.reshape(sources * CORES, share, half),
        ("fs", "core"),
        split_axis=0,
        concat_axis=0,
        tiled=True,
    )
    take, share = pl.pallas_call(
        functools.partial(place_kernel, experts=experts, capacity=capacity),
        out_shape=(
            jax.ShapeDtypeStruct((n * top, experts * capacity), BF16),
            jax.ShapeDtypeStruct((n * top, half), F32),
        ),
        in_specs=[vmem] * 2,
        out_specs=(vmem, vmem),
        compiler_params=PARAMS,
        name="place",
    )(choice, ratio)
    out = pl.pallas_call(
        pick_kernel,
        out_shape=jax.ShapeDtypeStruct((n * top, half), BF16),
        in_specs=[vmem] * 3,
        out_specs=vmem,
        compiler_params=PARAMS,
        name="pick",
    )(back.reshape(experts * capacity, half), take, share)
    return (
        gate.reshape(1, sources * block, half),
        up.reshape(1, sources * block, half),
        out.reshape(n, top, half),
    )


def solution(mesh):
    groups, sources, total = (mesh.shape[a] for a in ("grp", "fs", "tp"))
    devices = mesh.devices.reshape(groups, sources, total // CORES, CORES)
    tp = ("x", "core")
    return jax.shard_map(
        on_device,
        mesh=jax.sharding.Mesh(devices, ("grp", "fs", *tp)),
        in_specs=(
            P(("grp", "fs"), None),
            P("fs"),
            P(None, "fs", tp),
            P(None, "fs", tp),
            P(("grp", "fs"), None),
            P(("grp", "fs"), None),
        ),
        out_specs=(
            P(("grp", "fs"), None, tp),
            P(("grp", "fs"), None, tp),
            P(("grp", "fs"), None, tp),
        ),
        check_vma=False,
    )
```

```python
import functools
import jax
import jax.numpy as jnp
from jax import lax
from jax.experimental import pallas as pl
from jax.experimental.pallas import tpu as pltpu
from jax.sharding import PartitionSpec as P

F32 = jnp.float32
BF16 = jnp.bfloat16
CORES = 2
TILE = 8
PARTS = 4
PARAMS = pltpu.CompilerParams(vmem_limit_bytes=16 << 20)


def iota(shape, dim):
    return lax.broadcasted_iota(jnp.int32, shape, dim)


def dot(a, b, dims=(((1,), (0,)), ((), ()))):
    return lax.dot_general(a, b, dims, preferred_element_type=F32)


def column(row):
    n = row.shape[1]
    return jnp.sum(jnp.where(iota((n, n), 0) == iota((n, n), 1), row, 0.0), axis=1, keepdims=True)


def slots_of(choice, experts):
    top, n = choice.shape
    expert = iota((experts, n), 0).astype(F32)
    named = jnp.zeros((experts, n), F32)
    for k in range(top):
        named = named + (choice[k : k + 1, :] == expert).astype(F32)
    before = (iota((n, n), 0) < iota((n, n), 1)).astype(F32).astype(BF16)
    return named, dot(named.astype(BF16), before)


def pack_kernel(
    tokens, chosen, gain, gate, up, out, tok, cho, gai, gat, upp, gains, sems, *, experts, capacity
):
    n, width = tok.shape
    narrow = out.shape[2]
    piece, half = gat.shape[1:]
    share = capacity // CORES
    part = n // PARTS
    mine = pl.multiple_of(lax.axis_index("grp") * piece, TILE)
    pairs = [(chosen, cho), (gain, gai)]
    pairs += [(tokens.at[pl.ds(i * part, part)], tok.at[pl.ds(i * part, part)]) for i in range(PARTS)]
    pairs += [(gate.at[:, pl.ds(mine, piece), :], gat), (up.at[:, pl.ds(mine, piece), :], upp)]
    copies = [pltpu.make_async_copy(a, b, sems.at[i]) for i, (a, b) in enumerate(pairs)]
    for c in copies:
        c.start()
    copies[0].wait()
    named, slot = slots_of(cho[...].astype(F32), experts)
    slot = jnp.where(named > 0, slot, -1.0)
    first = lax.axis_index("core") * share
    pick = slot[:, None, :] == (iota((experts, share, n), 1) + first).astype(F32)
    pick = pick.astype(F32).reshape(experts * share, n).astype(BF16)
    copies[1].wait()
    gains[...] = jnp.broadcast_to(column(gai[...]), gains.shape)
    for c in copies[2 : 2 + PARTS]:
        c.wait()
    x = tok[...].astype(F32)
    scale = lax.rsqrt(jnp.sum(x * x, axis=-1, keepdims=True) / width + 1e-06)
    for c in range(CORES):
        at = pl.multiple_of((lax.axis_index("x") * CORES + c) * narrow, narrow)
        own = (tok[:, pl.ds(at, narrow)].astype(F32) * scale).astype(BF16)
        rows = dot(pick, own).astype(BF16).reshape(experts, share, narrow)
        out[:, c * share : (c + 1) * share, :] = rows
    for c in copies[2 + PARTS :]:
        c.wait()
    g = gains[pl.ds(mine, piece), :][None]
    out[:, capacity:, :half] = (gat[...] * g).astype(BF16)
    out[:, capacity:, half:] = (upp[...] * g).astype(BF16)


def assemble_kernel(*refs, parts, chips):
    gate, up, mixed = refs[-3:]
    weights, others = refs[:parts], refs[parts:-3]
    half = gate.shape[2]
    narrow = 2 * half
    rows = mixed.shape[1]
    piece = weights[0].shape[2]
    mine = lax.axis_index("grp")
    x = lax.axis_index("x")
    core = lax.axis_index("core")
    chip = [place(x, core, chips) for place in chip_places(chips)]
    for side, group in enumerate((weights, others)):
        q = 0
        for ref in group:
            for j in range(ref.shape[0]):
                at = pl.multiple_of((mine ^ q) * piece, TILE)
                if side == 0:
                    gate[:, pl.ds(at, piece), :] = ref[j, :, :, :half]
                    up[:, pl.ds(at, piece), :] = ref[j, :, :, half:]
                for i, c in enumerate(chip):
                    part = ref[j, pl.ds(c * rows, rows)]
                    mixed[i, :, pl.ds(at, piece), side * narrow : (side + 1) * narrow] = part
                q += 1


def expert_kernel(mixed, *refs):
    hidden, slices = refs[-1], refs[:-1]
    half = hidden.shape[3]
    slots, narrow = slices[0].shape[1:]
    share = slots // CORES
    per = mixed.shape[1] // CORES
    block = mixed.shape[2]
    core = lax.axis_index("core")
    a = None
    for i, ref in enumerate(slices):
        for c in range(CORES):
            rows = ref[:, c * share : (c + 1) * share, :].reshape(-1, narrow)
            w = mixed[i, c * per : (c + 1) * per].reshape(per * block, CORES * narrow)
            d = dot(rows, w)
            a = d if a is None else a + d
    for side, to in enumerate((core, 1 - core)):
        g = a[:, side * narrow : side * narrow + half]
        u = a[:, side * narrow + half : (side + 1) * narrow]
        h = (g / (1.0 + jnp.exp(-g)) * u).astype(BF16)
        hidden[:, pl.ds(to, 1)] = h.reshape(hidden.shape[0], 1, share, half)


def place_kernel(chosen, affinity, take, share, *, experts, capacity):
    top, n = chosen.shape
    lines, total = take.shape
    choice = chosen[...].astype(F32)
    _, slot = slots_of(choice, experts)
    expert = iota((experts, n), 0).astype(F32)
    a = affinity[...]
    part = a / jnp.sum(a, axis=0, keepdims=True)
    line = iota((lines, n), 0)
    here = line // top == iota((lines, n), 1)
    at = jnp.zeros((lines, n), F32)
    of = jnp.zeros((lines, n), F32)
    for k in range(top):
        c = choice[k : k + 1, :]
        goal = jnp.sum(jnp.where(c == expert, slot, 0.0), axis=0, keepdims=True) + c * capacity
        this = here & (line % top == k)
        at = jnp.where(this, goal, at)
        of = jnp.where(this, part[k : k + 1, :], of)
    at = jnp.sum(at, axis=1, keepdims=True)
    take[...] = (iota((lines, total), 1).astype(F32) == at).astype(F32).astype(BF16)
    share[...] = jnp.broadcast_to(jnp.sum(of, axis=1, keepdims=True), share.shape)


def pick_kernel(back, take, share, out):
    out[...] = (dot(take[...], back[...]) * share[...]).astype(BF16)


def chip_places(chips):
    def away(steps):
        return lambda x, core, n: (x + jnp.where(core == 0, -steps, steps) + n) % n

    places = [away(0)]
    for s in range(1, chips // 2 + 1):
        places.append(away(s))
        if s <= (chips - 1) // 2:
            places.append(away(-s))
    return places


def gather_slices(own, chips):
    def hop(sign):
        def to(x, c):
            return (x + (sign if c == 0 else -sign)) % chips

        pairs = [(x, c) for x in range(chips) for c in range(CORES)]
        return [(x * CORES + c, to(x, c) * CORES + c) for x, c in pairs]

    got = [own]
    one = two = own
    for s in range(1, chips // 2 + 1):
        one = lax.ppermute(one, ("x", "core"), hop(1))
        got.append(one)
        if s <= (chips - 1) // 2:
            two = lax.ppermute(two, ("x", "core"), hop(-1))
            got.append(two)
    return got


def gather_groups(own, groups):
    got = [own]
    step = 1
    while step < groups:
        send = got[0] if len(got) == 1 else jnp.concatenate(got, axis=0)
        table = [(i, i ^ step) for i in range(groups)]
        got.append(lax.ppermute(send, "grp", table))
        step *= 2
    return got


def on_device(tokens, norm_gain, gate_master, up_master, chosen, affinity):
    groups, sources, chips = (lax.axis_size(a) for a in ("grp", "fs", "x"))
    total = chips * CORES
    experts, block, half = gate_master.shape
    n, width = tokens.shape
    top = chosen.shape[1]
    capacity = n * top * 2 // experts
    narrow = width // total
    piece = block // groups
    vmem = pl.BlockSpec(memory_space=pltpu.VMEM)

    sent = pl.pallas_call(
        functools.partial(pack_kernel, experts=experts, capacity=capacity),
        out_shape=jax.ShapeDtypeStruct((experts, capacity + piece, narrow), BF16),
        in_specs=[pl.BlockSpec(memory_space=pltpu.HBM)] * 5,
        out_specs=vmem,
        scratch_shapes=[
            pltpu.VMEM((n, width), BF16),
            pltpu.VMEM((top, n), jnp.int32),
            pltpu.VMEM((1, block), F32),
            pltpu.VMEM((experts, piece, half), F32),
            pltpu.VMEM((experts, piece, half), F32),
            pltpu.VMEM((block, half), F32),
            pltpu.SemaphoreType.DMA((PARTS + 4,)),
        ],
        compiler_params=PARAMS,
        name="pack",
    )(*(
        pltpu.with_memory_space_constraint(a, pltpu.HBM)
        for a in (tokens, chosen.T, norm_gain[None, :], gate_master, up_master)
    ))
    got = lax.all_to_all(sent, "fs", split_axis=0, concat_axis=0, tiled=True)
    rows = got[:, :capacity, :]
    weights = gather_groups(got[None, :, capacity:, :], groups)
    slices = gather_slices(rows, chips)
    swap = [(c, 1 - c) for c in range(CORES)]
    others = [lax.ppermute(w, "core", swap) for w in weights]
    share = capacity // CORES

    gate, up, mixed = pl.pallas_call(
        functools.partial(assemble_kernel, parts=len(weights), chips=chips),
        out_shape=(
            jax.ShapeDtypeStruct((sources, block, half), BF16),
            jax.ShapeDtypeStruct((sources, block, half), BF16),
            pltpu.VMEM((chips, CORES * sources // total, block, CORES * narrow), BF16),
        ),
        in_specs=[vmem] * (2 * len(weights)),
        out_specs=(vmem, vmem, vmem),
        compiler_params=PARAMS,
        name="assemble",
    )(*weights, *others)
    hidden = pl.pallas_call(
        expert_kernel,
        out_shape=pltpu.VMEM((sources, CORES, share, half), BF16),
        in_specs=[vmem] * (1 + len(slices)),
        out_specs=vmem,
        compiler_params=PARAMS,
        name="experts",
    )(mixed, *slices)
    hidden, choice, ratio = lax.optimization_barrier((hidden, chosen.T, affinity.T))
    back = lax.all_to_all(
        hidden.reshape(sources * CORES, share, half),
        ("fs", "core"),
        split_axis=0,
        concat_axis=0,
        tiled=True,
    )
    take, share = pl.pallas_call(
        functools.partial(place_kernel, experts=experts, capacity=capacity),
        out_shape=(
            jax.ShapeDtypeStruct((n * top, experts * capacity), BF16),
            jax.ShapeDtypeStruct((n * top, half), F32),
        ),
        in_specs=[vmem] * 2,
        out_specs=(vmem, vmem),
        compiler_params=PARAMS,
        name="place",
    )(choice, ratio)
    out = pl.pallas_call(
        pick_kernel,
        out_shape=jax.ShapeDtypeStruct((n * top, half), BF16),
        in_specs=[vmem] * 3,
        out_specs=vmem,
        compiler_params=PARAMS,
        name="pick",
    )(back.reshape(experts * capacity, half), take, share)
    return (
        gate.reshape(1, sources * block, half),
        up.reshape(1, sources * block, half),
        out.reshape(n, top, half),
    )


def solution(mesh):
    groups, sources, total = (mesh.shape[a] for a in ("grp", "fs", "tp"))
    devices = mesh.devices.reshape(groups, sources, total // CORES, CORES)
    tp = ("x", "core")
    return jax.shard_map(
        on_device,
        mesh=jax.sharding.Mesh(devices, ("grp", "fs", *tp)),
        in_specs=(
            P(("grp", "fs"), None),
            P("fs"),
            P(None, "fs", tp),
            P(None, "fs", tp),
            P(("grp", "fs"), None),
            P(("grp", "fs"), None),
        ),
        out_specs=(
            P(("grp", "fs"), None, tp),
            P(("grp", "fs"), None, tp),
            P(("grp", "fs"), None, tp),
        ),
        check_vma=False,
    )
```

```python
import functools
import jax
import jax.numpy as jnp
from jax import lax
from jax.experimental import pallas as pl
from jax.experimental.pallas import tpu as pltpu
from jax.sharding import PartitionSpec as P

F32 = jnp.float32
BF16 = jnp.bfloat16
CORES = 2
TILE = 8
PARTS = 4
PARAMS = pltpu.CompilerParams(vmem_limit_bytes=16 << 20)


def iota(shape, dim):
    return lax.broadcasted_iota(jnp.int32, shape, dim)


def dot(a, b, dims=(((1,), (0,)), ((), ()))):
    return lax.dot_general(a, b, dims, preferred_element_type=F32)


def column(row):
    n = row.shape[1]
    return jnp.sum(jnp.where(iota((n, n), 0) == iota((n, n), 1), row, 0.0), axis=1, keepdims=True)


def slots_of(choice, experts):
    top, n = choice.shape
    expert = iota((experts, n), 0).astype(F32)
    named = jnp.zeros((experts, n), F32)
    for k in range(top):
        named = named + (choice[k : k + 1, :] == expert).astype(F32)
    before = (iota((n, n), 0) < iota((n, n), 1)).astype(F32).astype(BF16)
    return named, dot(named.astype(BF16), before)


def pack_kernel(
    tokens, chosen, gain, gate, up, out, tok, cho, gai, gat, upp, gains, sems, *, experts, capacity
):
    n, width = tok.shape
    narrow = out.shape[2]
    piece, half = gat.shape[1:]
    share = capacity // CORES
    part = n // PARTS
    mine = pl.multiple_of(lax.axis_index("grp") * piece, TILE)
    pairs = [(chosen, cho), (gain, gai)]
    pairs += [(tokens.at[pl.ds(i * part, part)], tok.at[pl.ds(i * part, part)]) for i in range(PARTS)]
    pairs += [(gate.at[:, pl.ds(mine, piece), :], gat), (up.at[:, pl.ds(mine, piece), :], upp)]
    copies = [pltpu.make_async_copy(a, b, sems.at[i]) for i, (a, b) in enumerate(pairs)]
    for c in copies:
        c.start()
    copies[0].wait()
    named, slot = slots_of(cho[...].astype(F32), experts)
    slot = jnp.where(named > 0, slot, -1.0)
    first = lax.axis_index("core") * share
    pick = slot[:, None, :] == (iota((experts, share, n), 1) + first).astype(F32)
    pick = pick.astype(F32).reshape(experts * share, n).astype(BF16)
    copies[1].wait()
    gains[...] = jnp.broadcast_to(column(gai[...]), gains.shape)
    for c in copies[2 : 2 + PARTS]:
        c.wait()
    x = tok[...].astype(F32)
    scale = lax.rsqrt(jnp.sum(x * x, axis=-1, keepdims=True) / width + 1e-06)
    for c in range(CORES):
        at = pl.multiple_of((lax.axis_index("x") * CORES + c) * narrow, narrow)
        own = (tok[:, pl.ds(at, narrow)].astype(F32) * scale).astype(BF16)
        rows = dot(pick, own).astype(BF16).reshape(experts, share, narrow)
        out[:, c * share : (c + 1) * share, :] = rows
    for c in copies[2 + PARTS :]:
        c.wait()
    g = gains[pl.ds(mine, piece), :][None]
    out[:, capacity:, :half] = (gat[...] * g).astype(BF16)
    out[:, capacity:, half:] = (upp[...] * g).astype(BF16)


def assemble_kernel(*refs, parts, chips):
    gate, up, mixed = refs[-3:]
    weights, others = refs[:parts], refs[parts:-3]
    half = gate.shape[2]
    narrow = 2 * half
    rows = mixed.shape[1]
    piece = weights[0].shape[2]
    mine = lax.axis_index("grp")
    x = lax.axis_index("x")
    core = lax.axis_index("core")
    chip = [place(x, core, chips) for place in chip_places(chips)]
    for side, group in enumerate((weights, others)):
        q = 0
        for ref in group:
            for j in range(ref.shape[0]):
                at = pl.multiple_of((mine ^ q) * piece, TILE)
                if side == 0:
                    gate[:, pl.ds(at, piece), :] = ref[j, :, :, :half]
                    up[:, pl.ds(at, piece), :] = ref[j, :, :, half:]
                for i, c in enumerate(chip):
                    part = ref[j, pl.ds(c * rows, rows)]
                    mixed[i, :, pl.ds(at, piece), side * narrow : (side + 1) * narrow] = part
                q += 1


def expert_kernel(mixed, *refs):
    hidden, slices = refs[-1], refs[:-1]
    half = hidden.shape[3]
    slots, narrow = slices[0].shape[1:]
    share = slots // CORES
    per = mixed.shape[1] // CORES
    block = mixed.shape[2]
    core = lax.axis_index("core")
    a = None
    for i, ref in enumerate(slices):
        for c in range(CORES):
            rows = ref[:, c * share : (c + 1) * share, :].reshape(-1, narrow)
            w = mixed[i, c * per : (c + 1) * per].reshape(per * block, CORES * narrow)
            d = dot(rows, w)
            a = d if a is None else a + d
    for side, to in enumerate((core, 1 - core)):
        g = a[:, side * narrow : side * narrow + half]
        u = a[:, side * narrow + half : (side + 1) * narrow]
        h = (g / (1.0 + jnp.exp(-g)) * u).astype(BF16)
        h = h.reshape(hidden.shape[0], 1, share, half)
        turn = hidden.shape[0] // 2
        hidden[:turn, pl.ds(to, 1)] = h[turn:]
        hidden[turn:, pl.ds(to, 1)] = h[:turn]


def place_kernel(chosen, affinity, take, share, *, experts, capacity):
    top, n = chosen.shape
    lines, total = take.shape
    choice = chosen[...].astype(F32)
    _, slot = slots_of(choice, experts)
    expert = iota((experts, n), 0).astype(F32)
    turn = experts // 2
    a = affinity[...]
    part = a / jnp.sum(a, axis=0, keepdims=True)
    line = iota((lines, n), 0)
    here = line // top == iota((lines, n), 1)
    at = jnp.zeros((lines, n), F32)
    of = jnp.zeros((lines, n), F32)
    for k in range(top):
        c = choice[k : k + 1, :]
        place = jnp.where(c < turn, c + turn, c - turn)
        goal = jnp.sum(jnp.where(c == expert, slot, 0.0), axis=0, keepdims=True) + place * capacity
        this = here & (line % top == k)
        at = jnp.where(this, goal, at)
        of = jnp.where(this, part[k : k + 1, :], of)
    at = jnp.sum(at, axis=1, keepdims=True)
    take[...] = (iota((lines, total), 1).astype(F32) == at).astype(F32).astype(BF16)
    share[...] = jnp.broadcast_to(jnp.sum(of, axis=1, keepdims=True), share.shape)


def pick_kernel(back, take, share, out):
    out[...] = (dot(take[...], back[...]) * share[...]).astype(BF16)


def chip_places(chips):
    def away(steps):
        return lambda x, core, n: (x + jnp.where(core == 0, -steps, steps) + n) % n

    places = [away(0)]
    for s in range(1, chips // 2 + 1):
        places.append(away(s))
        if s <= (chips - 1) // 2:
            places.append(away(-s))
    return places


def gather_slices(own, chips):
    def hop(sign):
        def to(x, c):
            return (x + (sign if c == 0 else -sign)) % chips

        pairs = [(x, c) for x in range(chips) for c in range(CORES)]
        return [(x * CORES + c, to(x, c) * CORES + c) for x, c in pairs]

    got = [own]
    one = two = own
    for s in range(1, chips // 2 + 1):
        one = lax.ppermute(one, ("x", "core"), hop(1))
        got.append(one)
        if s <= (chips - 1) // 2:
            two = lax.ppermute(two, ("x", "core"), hop(-1))
            got.append(two)
    return got


def gather_groups(own, groups):
    got = [own]
    step = 1
    while step < groups:
        send = got[0] if len(got) == 1 else jnp.concatenate(got, axis=0)
        table = [(i, i ^ step) for i in range(groups)]
        got.append(lax.ppermute(send, "grp", table))
        step *= 2
    return got


def on_device(tokens, norm_gain, gate_master, up_master, chosen, affinity):
    groups, sources, chips = (lax.axis_size(a) for a in ("grp", "fs", "x"))
    total = chips * CORES
    experts, block, half = gate_master.shape
    n, width = tokens.shape
    top = chosen.shape[1]
    capacity = n * top * 2 // experts
    narrow = width // total
    piece = block // groups
    vmem = pl.BlockSpec(memory_space=pltpu.VMEM)

    sent = pl.pallas_call(
        functools.partial(pack_kernel, experts=experts, capacity=capacity),
        out_shape=jax.ShapeDtypeStruct((experts, capacity + piece, narrow), BF16),
        in_specs=[pl.BlockSpec(memory_space=pltpu.HBM)] * 5,
        out_specs=vmem,
        scratch_shapes=[
            pltpu.VMEM((n, width), BF16),
            pltpu.VMEM((top, n), jnp.int32),
            pltpu.VMEM((1, block), F32),
            pltpu.VMEM((experts, piece, half), F32),
            pltpu.VMEM((experts, piece, half), F32),
            pltpu.VMEM((block, half), F32),
            pltpu.SemaphoreType.DMA((PARTS + 4,)),
        ],
        compiler_params=PARAMS,
        name="pack",
    )(*(
        pltpu.with_memory_space_constraint(a, pltpu.HBM)
        for a in (tokens, chosen.T, norm_gain[None, :], gate_master, up_master)
    ))
    got = lax.all_to_all(sent, "fs", split_axis=0, concat_axis=0, tiled=True)
    rows = got[:, :capacity, :]
    weights = gather_groups(got[None, :, capacity:, :], groups)
    slices = gather_slices(rows, chips)
    swap = [(c, 1 - c) for c in range(CORES)]
    others = [lax.ppermute(w, "core", swap) for w in weights]
    share = capacity // CORES

    gate, up, mixed = pl.pallas_call(
        functools.partial(assemble_kernel, parts=len(weights), chips=chips),
        out_shape=(
            jax.ShapeDtypeStruct((sources, block, half), BF16),
            jax.ShapeDtypeStruct((sources, block, half), BF16),
            pltpu.VMEM((chips, CORES * sources // total, block, CORES * narrow), BF16),
        ),
        in_specs=[vmem] * (2 * len(weights)),
        out_specs=(vmem, vmem, vmem),
        compiler_params=PARAMS,
        name="assemble",
    )(*weights, *others)
    hidden = pl.pallas_call(
        expert_kernel,
        out_shape=pltpu.VMEM((sources, CORES, share, half), BF16),
        in_specs=[vmem] * (1 + len(slices)),
        out_specs=vmem,
        compiler_params=PARAMS,
        name="experts",
    )(mixed, *slices)
    hidden, choice, ratio = lax.optimization_barrier((hidden, chosen.T, affinity.T))
    turn = sources // 2
    order = [(z + turn) % sources * CORES + c for z in range(sources) for c in range(CORES)]
    back = lax.all_to_all(
        hidden.reshape(sources * CORES, share, half),
        ("fs", "core"),
        split_axis=0,
        concat_axis=0,
        axis_index_groups=[order],
        tiled=True,
    )
    take, share = pl.pallas_call(
        functools.partial(place_kernel, experts=experts, capacity=capacity),
        out_shape=(
            jax.ShapeDtypeStruct((n * top, experts * capacity), BF16),
            jax.ShapeDtypeStruct((n * top, half), F32),
        ),
        in_specs=[vmem] * 2,
        out_specs=(vmem, vmem),
        compiler_params=PARAMS,
        name="place",
    )(choice, ratio)
    out = pl.pallas_call(
        pick_kernel,
        out_shape=jax.ShapeDtypeStruct((n * top, half), BF16),
        in_specs=[vmem] * 3,
        out_specs=vmem,
        compiler_params=PARAMS,
        name="pick",
    )(back.reshape(experts * capacity, half), take, share)
    return (
        gate.reshape(1, sources * block, half),
        up.reshape(1, sources * block, half),
        out.reshape(n, top, half),
    )


def solution(mesh):
    groups, sources, total = (mesh.shape[a] for a in ("grp", "fs", "tp"))
    devices = mesh.devices.reshape(groups, sources, total // CORES, CORES)
    tp = ("x", "core")
    return jax.shard_map(
        on_device,
        mesh=jax.sharding.Mesh(devices, ("grp", "fs", *tp)),
        in_specs=(
            P(("grp", "fs"), None),
            P("fs"),
            P(None, "fs", tp),
            P(None, "fs", tp),
            P(("grp", "fs"), None),
            P(("grp", "fs"), None),
        ),
        out_specs=(
            P(("grp", "fs"), None, tp),
            P(("grp", "fs"), None, tp),
            P(("grp", "fs"), None, tp),
        ),
        check_vma=False,
    )
```

```python
import functools
import jax
import jax.numpy as jnp
from jax import lax
from jax.experimental import pallas as pl
from jax.experimental.pallas import tpu as pltpu
from jax.sharding import PartitionSpec as P

F32 = jnp.float32
BF16 = jnp.bfloat16
CORES = 2
TILE = 8
PARTS = 4
PARAMS = pltpu.CompilerParams(vmem_limit_bytes=16 << 20)


def iota(shape, dim):
    return lax.broadcasted_iota(jnp.int32, shape, dim)


def dot(a, b, dims=(((1,), (0,)), ((), ()))):
    return lax.dot_general(a, b, dims, preferred_element_type=F32)


def column(row):
    n = row.shape[1]
    return jnp.sum(jnp.where(iota((n, n), 0) == iota((n, n), 1), row, 0.0), axis=1, keepdims=True)


def slots_of(choice, experts):
    top, n = choice.shape
    expert = iota((experts, n), 0).astype(F32)
    named = jnp.zeros((experts, n), F32)
    for k in range(top):
        named = named + (choice[k : k + 1, :] == expert).astype(F32)
    before = (iota((n, n), 0) < iota((n, n), 1)).astype(F32).astype(BF16)
    return named, dot(named.astype(BF16), before)


def pack_kernel(
    tokens, chosen, gain, gate, up, out, tok, cho, gai, gat, upp, gains, mine_rows, sems, *, experts, capacity
):
    n, width = tok.shape
    narrow = out.shape[2]
    piece, half = gat.shape[1:]
    share = capacity // CORES
    part = n // PARTS
    mine = pl.multiple_of(lax.axis_index("grp") * piece, TILE)
    pairs = [(chosen, cho), (gain, gai)]
    pairs += [(tokens.at[pl.ds(i * part, part)], tok.at[pl.ds(i * part, part)]) for i in range(PARTS)]
    pairs += [(gate.at[:, pl.ds(mine, piece), :], gat), (up.at[:, pl.ds(mine, piece), :], upp)]
    copies = [pltpu.make_async_copy(a, b, sems.at[i]) for i, (a, b) in enumerate(pairs)]
    for c in copies:
        c.start()
    copies[0].wait()
    named, slot = slots_of(cho[...].astype(F32), experts)
    slot = jnp.where(named > 0, slot, -1.0)
    first = lax.axis_index("core") * share
    pick = slot[:, None, :] == (iota((experts, share, n), 1) + first).astype(F32)
    pick = pick.astype(F32).reshape(experts * share, n).astype(BF16)
    copies[1].wait()
    gains[...] = jnp.broadcast_to(column(gai[...]), gains.shape)
    for i in range(PARTS):
        copies[2 + i].wait()
        x = tok[i * part : (i + 1) * part].astype(F32)
        scale = lax.rsqrt(jnp.sum(x * x, axis=-1, keepdims=True) / width + 1e-06)
        for c in range(CORES):
            at = pl.multiple_of((lax.axis_index("x") * CORES + c) * narrow, narrow)
            own = tok[i * part : (i + 1) * part, pl.ds(at, narrow)].astype(F32)
            mine_rows[c, i * part : (i + 1) * part, :] = (own * scale).astype(BF16)
    for c in range(CORES):
        rows = dot(pick, mine_rows[c]).astype(BF16).reshape(experts, share, narrow)
        out[:, c * share : (c + 1) * share, :] = rows
    for c in copies[2 + PARTS :]:
        c.wait()
    g = gains[pl.ds(mine, piece), :][None]
    out[:, capacity:, :half] = (gat[...] * g).astype(BF16)
    out[:, capacity:, half:] = (upp[...] * g).astype(BF16)


def assemble_kernel(*refs, parts, chips):
    gate, up, mixed = refs[-3:]
    weights, others = refs[:parts], refs[parts:-3]
    half = gate.shape[2]
    narrow = 2 * half
    rows = mixed.shape[1]
    piece = weights[0].shape[2]
    mine = lax.axis_index("grp")
    x = lax.axis_index("x")
    core = lax.axis_index("core")
    chip = [place(x, core, chips) for place in chip_places(chips)]
    for side, group in enumerate((weights, others)):
        q = 0
        for ref in group:
            for j in range(ref.shape[0]):
                at = pl.multiple_of((mine ^ q) * piece, TILE)
                if side == 0:
                    gate[:, pl.ds(at, piece), :] = ref[j, :, :, :half]
                    up[:, pl.ds(at, piece), :] = ref[j, :, :, half:]
                for i, c in enumerate(chip):
                    part = ref[j, pl.ds(c * rows, rows)]
                    mixed[i, :, pl.ds(at, piece), side * narrow : (side + 1) * narrow] = part
                q += 1


def expert_kernel(mixed, *refs):
    hidden, slices = refs[-1], refs[:-1]
    half = hidden.shape[3]
    slots, narrow = slices[0].shape[1:]
    share = slots // CORES
    per = mixed.shape[1] // CORES
    block = mixed.shape[2]
    core = lax.axis_index("core")
    a = None
    for i, ref in enumerate(slices):
        for c in range(CORES):
            rows = ref[:, c * share : (c + 1) * share, :].reshape(-1, narrow)
            w = mixed[i, c * per : (c + 1) * per].reshape(per * block, CORES * narrow)
            d = dot(rows, w)
            a = d if a is None else a + d
    for side, to in enumerate((core, 1 - core)):
        g = a[:, side * narrow : side * narrow + half]
        u = a[:, side * narrow + half : (side + 1) * narrow]
        h = (g / (1.0 + jnp.exp(-g)) * u).astype(BF16)
        h = h.reshape(hidden.shape[0], 1, share, half)
        turn = hidden.shape[0] // 2
        hidden[:turn, pl.ds(to, 1)] = h[turn:]
        hidden[turn:, pl.ds(to, 1)] = h[:turn]


def place_kernel(chosen, affinity, take, share, *, experts, capacity):
    top, n = chosen.shape
    lines, total = take.shape
    choice = chosen[...].astype(F32)
    _, slot = slots_of(choice, experts)
    expert = iota((experts, n), 0).astype(F32)
    turn = experts // 2
    a = affinity[...]
    part = a / jnp.sum(a, axis=0, keepdims=True)
    line = iota((lines, n), 0)
    here = line // top == iota((lines, n), 1)
    at = jnp.zeros((lines, n), F32)
    of = jnp.zeros((lines, n), F32)
    for k in range(top):
        c = choice[k : k + 1, :]
        place = jnp.where(c < turn, c + turn, c - turn)
        goal = jnp.sum(jnp.where(c == expert, slot, 0.0), axis=0, keepdims=True) + place * capacity
        this = here & (line % top == k)
        at = jnp.where(this, goal, at)
        of = jnp.where(this, part[k : k + 1, :], of)
    at = jnp.sum(at, axis=1, keepdims=True)
    take[...] = (iota((lines, total), 1).astype(F32) == at).astype(F32).astype(BF16)
    share[...] = jnp.broadcast_to(jnp.sum(of, axis=1, keepdims=True), share.shape)


def pick_kernel(back, take, share, out):
    out[...] = (dot(take[...], back[...]) * share[...]).astype(BF16)


def chip_places(chips):
    def away(steps):
        return lambda x, core, n: (x + jnp.where(core == 0, -steps, steps) + n) % n

    places = [away(0)]
    for s in range(1, chips // 2 + 1):
        places.append(away(s))
        if s <= (chips - 1) // 2:
            places.append(away(-s))
    return places


def gather_slices(own, chips):
    def hop(sign):
        def to(x, c):
            return (x + (sign if c == 0 else -sign)) % chips

        pairs = [(x, c) for x in range(chips) for c in range(CORES)]
        return [(x * CORES + c, to(x, c) * CORES + c) for x, c in pairs]

    got = [own]
    one = two = own
    for s in range(1, chips // 2 + 1):
        one = lax.ppermute(one, ("x", "core"), hop(1))
        got.append(one)
        if s <= (chips - 1) // 2:
            two = lax.ppermute(two, ("x", "core"), hop(-1))
            got.append(two)
    return got


def gather_groups(own, groups):
    got = [own]
    step = 1
    while step < groups:
        send = got[0] if len(got) == 1 else jnp.concatenate(got, axis=0)
        table = [(i, i ^ step) for i in range(groups)]
        got.append(lax.ppermute(send, "grp", table))
        step *= 2
    return got


def on_device(tokens, norm_gain, gate_master, up_master, chosen, affinity):
    groups, sources, chips = (lax.axis_size(a) for a in ("grp", "fs", "x"))
    total = chips * CORES
    experts, block, half = gate_master.shape
    n, width = tokens.shape
    top = chosen.shape[1]
    capacity = n * top * 2 // experts
    narrow = width // total
    piece = block // groups
    vmem = pl.BlockSpec(memory_space=pltpu.VMEM)

    sent = pl.pallas_call(
        functools.partial(pack_kernel, experts=experts, capacity=capacity),
        out_shape=jax.ShapeDtypeStruct((experts, capacity + piece, narrow), BF16),
        in_specs=[pl.BlockSpec(memory_space=pltpu.HBM)] * 5,
        out_specs=vmem,
        scratch_shapes=[
            pltpu.VMEM((n, width), BF16),
            pltpu.VMEM((top, n), jnp.int32),
            pltpu.VMEM((1, block), F32),
            pltpu.VMEM((experts, piece, half), F32),
            pltpu.VMEM((experts, piece, half), F32),
            pltpu.VMEM((block, half), F32),
            pltpu.VMEM((CORES, n, narrow), BF16),
            pltpu.SemaphoreType.DMA((PARTS + 4,)),
        ],
        compiler_params=PARAMS,
        name="pack",
    )(*(
        pltpu.with_memory_space_constraint(a, pltpu.HBM)
        for a in (tokens, chosen.T, norm_gain[None, :], gate_master, up_master)
    ))
    got = lax.all_to_all(sent, "fs", split_axis=0, concat_axis=0, tiled=True)
    rows = got[:, :capacity, :]
    weights = gather_groups(got[None, :, capacity:, :], groups)
    slices = gather_slices(rows, chips)
    swap = [(c, 1 - c) for c in range(CORES)]
    others = [lax.ppermute(w, "core", swap) for w in weights]
    share = capacity // CORES

    gate, up, mixed = pl.pallas_call(
        functools.partial(assemble_kernel, parts=len(weights), chips=chips),
        out_shape=(
            jax.ShapeDtypeStruct((sources, block, half), BF16),
            jax.ShapeDtypeStruct((sources, block, half), BF16),
            pltpu.VMEM((chips, CORES * sources // total, block, CORES * narrow), BF16),
        ),
        in_specs=[vmem] * (2 * len(weights)),
        out_specs=(vmem, vmem, vmem),
        compiler_params=PARAMS,
        name="assemble",
    )(*weights, *others)
    hidden = pl.pallas_call(
        expert_kernel,
        out_shape=pltpu.VMEM((sources, CORES, share, half), BF16),
        in_specs=[vmem] * (1 + len(slices)),
        out_specs=vmem,
        compiler_params=PARAMS,
        name="experts",
    )(mixed, *slices)
    hidden, choice, ratio = lax.optimization_barrier((hidden, chosen.T, affinity.T))
    turn = sources // 2
    order = [(z + turn) % sources * CORES + c for z in range(sources) for c in range(CORES)]
    back = lax.all_to_all(
        hidden.reshape(sources * CORES, share, half),
        ("fs", "core"),
        split_axis=0,
        concat_axis=0,
        axis_index_groups=[order],
        tiled=True,
    )
    take, share = pl.pallas_call(
        functools.partial(place_kernel, experts=experts, capacity=capacity),
        out_shape=(
            jax.ShapeDtypeStruct((n * top, experts * capacity), BF16),
            jax.ShapeDtypeStruct((n * top, half), F32),
        ),
        in_specs=[vmem] * 2,
        out_specs=(vmem, vmem),
        compiler_params=PARAMS,
        name="place",
    )(choice, ratio)
    out = pl.pallas_call(
        pick_kernel,
        out_shape=jax.ShapeDtypeStruct((n * top, half), BF16),
        in_specs=[vmem] * 3,
        out_specs=vmem,
        compiler_params=PARAMS,
        name="pick",
    )(back.reshape(experts * capacity, half), take, share)
    return (
        gate.reshape(1, sources * block, half),
        up.reshape(1, sources * block, half),
        out.reshape(n, top, half),
    )


def solution(mesh):
    groups, sources, total = (mesh.shape[a] for a in ("grp", "fs", "tp"))
    devices = mesh.devices.reshape(groups, sources, total // CORES, CORES)
    tp = ("x", "core")
    return jax.shard_map(
        on_device,
        mesh=jax.sharding.Mesh(devices, ("grp", "fs", *tp)),
        in_specs=(
            P(("grp", "fs"), None),
            P("fs"),
            P(None, "fs", tp),
            P(None, "fs", tp),
            P(("grp", "fs"), None),
            P(("grp", "fs"), None),
        ),
        out_specs=(
            P(("grp", "fs"), None, tp),
            P(("grp", "fs"), None, tp),
            P(("grp", "fs"), None, tp),
        ),
        check_vma=False,
    )
```
